256 devices in a mesh: sp: 32 (over z, y), tp: 8 (over x, core).
Axes of the slice: x: 4, y: 4, z: 8, core: 2. Of those that a mesh axis runs over, the one named last changes fastest.
Arguments:
- hidden: bfloat16 [24576, 2048], P(('sp', 'tp')), may hold values from -6 to 6
- norm_gain: float32 [2, 2048], replicated, may hold values from 0.1 to 1.9
- w_value: bfloat16 [2, 2048, 2048], P(None, 'sp', 'tp'), may hold values from -0.125 to 0.125
- w_gate: bfloat16 [2, 2048, 2048], P(None, 'sp', 'tp'), may hold values from -0.125 to 0.125
- conv_weight: float32 [2, 31, 2048], P(None, None, 'tp'), may hold values from -3 to 3
- conv_bias: float32 [2, 2048], P(None, 'tp'), may hold values from -3 to 3
- chan_gain: float32 [2, 2048], P(None, 'tp'), may hold values from 0.1 to 1.9
- chan_shift: float32 [2, 2048], P(None, 'tp'), may hold values from -3 to 3
- w_out: bfloat16 [2, 2048, 2048], P(None, 'tp', 'sp'), may hold values from -0.125 to 0.125
Outputs:
- result: bfloat16 [24576, 2048], P(('sp', 'tp'))
The draws below stay inside these ranges and needn't reach their ends.
All inputs are finite; a program needn't handle non-finite values.
Results may differ from the reference program's by a relative error of at most 0.015.
Values may be sent and summed in bfloat16 or wider, within the bound.
No kernel may reach another device: no remote copies, remote signals or barrier semaphores. Data moves between devices by JAX's collectives and lax.ppermute only.
A program may use at most 64 MiB of HBM per device.

```python
import jax
import jax.numpy as jnp
from jax import lax

D = 2048
C = 2048
K = 31
LAYERS = 2
TOKENS = 24576
N_TP = 8


def draw_conv_weight(key, part):
    key_base = jax.random.fold_in(key, 11)
    key_perm = jax.random.fold_in(key, 12)
    base = jnp.clip(jax.random.normal(key_base, (LAYERS, K, C), jnp.float32), -4.0, 4.0)
    ladder = 0.3 * 10.0 ** (jnp.arange(8, dtype=jnp.float32) / 7.0)
    levels = jnp.stack([ladder[jax.random.permutation(jax.random.fold_in(key_perm, layer), 8)] for layer in range(LAYERS)])
    scales = jnp.repeat(levels, C // 8, axis=1)
    return base * K ** (-0.5) * scales[:, None, :]


def shard_levels(rng, dims, pieces, low, largest):
    level = 1.0
    for axis_at, shards_of in pieces:
        heights = jax.random.uniform(jax.random.fold_in(jax.random.fold_in(rng, 6), axis_at), (shards_of,), jnp.float32, low / len(pieces), largest / len(pieces))
        level = level * jnp.repeat(jnp.exp(heights), dims[axis_at] // shards_of).reshape((-1,) + (1,) * (len(dims) - 1 - axis_at))
    return level


def centred(own_key, shape, scale, reach, split=(), kind=jnp.bfloat16):
    level = shard_levels(own_key, shape, split, -0.22, 0.18) if split else 1.0
    drawn = jax.random.normal(own_key, shape, jnp.float32) * scale * level
    return jnp.minimum(jnp.maximum(drawn, -reach), reach).astype(kind)


def setup_inputs(seed: int = 0) -> dict:
    arg_keys = jax.random.split(jax.random.key(seed), 10)
    hidden = centred(arg_keys[0], (TOKENS, D), 1.0, 6.0, ((0, 256),))
    norm_gain = jnp.clip(1.0 + 0.18 * jax.random.normal(arg_keys[1], (LAYERS, D), jnp.float32), 0.1, 1.9)
    w_value = centred(arg_keys[2], (LAYERS, D, C), D ** -0.5, 0.125, ((1, 32), (2, 8)))
    w_gate = centred(arg_keys[3], (LAYERS, D, C), D ** -0.5, 0.125, ((1, 32), (2, 8)))
    conv_weight = draw_conv_weight(jax.random.fold_in(arg_keys[9], 71), 0)
    conv_bias = centred(arg_keys[5], (LAYERS, C), 0.5, 3.0, ((1, 8),), jnp.float32)
    chan_gain = jnp.clip(1.0 + 0.18 * jax.random.normal(arg_keys[6], (LAYERS, C), jnp.float32), 0.1, 1.9)
    chan_shift = centred(arg_keys[7], (LAYERS, C), 0.5, 3.0, ((1, 8),), jnp.float32)
    w_out = centred(arg_keys[8], (LAYERS, C, D), C ** -0.5, 0.125, ((1, 8), (2, 32)))
    return dict(hidden=hidden, norm_gain=norm_gain, w_value=w_value, w_gate=w_gate, conv_weight=conv_weight, conv_bias=conv_bias, chan_gain=chan_gain, chan_shift=chan_shift, w_out=w_out)


EPS = 1e-06

def reference(hidden, norm_gain, w_value, w_gate, conv_weight, conv_bias, chan_gain, chan_shift, w_out):
    state = hidden
    width = C // N_TP
    for layer in range(LAYERS):
        xf = state.astype(jnp.float32)
        scale = lax.rsqrt(lax.optimization_barrier(jnp.mean(xf * xf, axis=1, keepdims=True)) + EPS)
        normed = (xf * scale * norm_gain[layer][None, :]).astype(jnp.bfloat16)
        lin = jnp.dot(normed, w_value[layer], preferred_element_type=jnp.float32)
        gate = jnp.dot(normed, w_gate[layer], preferred_element_type=jnp.float32)
        glu = (lin * jax.nn.sigmoid(gate)).astype(jnp.bfloat16)
        padded = jnp.concatenate([jnp.zeros((K - 1, C), jnp.bfloat16), glu], axis=0).astype(jnp.float32)
        mixed = jnp.zeros((TOKENS, C), jnp.float32) + conv_bias[layer][None, :]
        for tap in range(K):
            mixed = mixed + conv_weight[layer, tap][None, :] * padded[tap:tap + TOKENS]
        mean = lax.optimization_barrier(jnp.mean(mixed, axis=1, keepdims=True))
        msq = lax.optimization_barrier(jnp.mean(mixed * mixed, axis=1, keepdims=True))
        var = msq - mean * mean
        act = jax.nn.silu((mixed - mean) * lax.rsqrt(var + EPS) * chan_gain[layer][None, :] + chan_shift[layer][None, :]).astype(jnp.bfloat16)
        update = jnp.zeros((TOKENS, D), jnp.float32)
        for block in range(N_TP):
            part = jnp.dot(act[:, block * width:(block + 1) * width], w_out[layer, block * width:(block + 1) * width, :], preferred_element_type=jnp.float32)
            part = lax.optimization_barrier(part.astype(jnp.bfloat16))
            update = update + part.astype(jnp.float32)
        state = (xf + update).astype(jnp.bfloat16)
    return state
```

```python
import jax
import jax.numpy as jnp
from jax import lax
from jax.sharding import Mesh
from jax.sharding import PartitionSpec as P

SP = ("z", "y")
SP_TP = ("z", "y", "x", "c")
EPS = 1e-06
BF = jnp.bfloat16
F32 = jnp.float32


def take(a, axis, by):
    n = lax.axis_size(axis)
    return lax.ppermute(a, axis, [((i + by) % n, i) for i in range(n)])


def swap(a):
    return lax.ppermute(a, "c", [(0, 1), (1, 0)])


def rolled(a, start, axis):
    return lax.dynamic_slice_in_dim(jnp.concatenate([a, a], axis=axis), start, a.shape[axis], axis)


def gather_rows(a):
    y = lax.axis_index("y")
    near = jnp.concatenate([a, take(a, "y", 1), take(a, "y", 2), take(a, "y", 3)], axis=0)
    rows = a.shape[0]
    near = rolled(near, ((4 - y) % 4) * rows, 0)
    half = near.shape[0] // 2
    p1, m1 = take(near, "z", 1), take(near, "z", -1)
    p2, m2 = take(p1, "z", 1), take(m1, "z", -1)
    p3, m3 = take(p2, "z", 1), take(m2, "z", -1)
    top, low = take(p3[:half], "z", 1), take(m3[half:], "z", -1)
    own = jnp.concatenate([near, p1, p2, p3, top, low, m3, m2, m1], axis=0)
    return own, swap(own)


def gather_tokens(h):
    half = h.shape[1] // 2
    left, right = h[:, :half], h[:, half:]
    m_left, p_right = take(left, "x", -1), take(right, "x", 1)
    m_right, p_left = take(right, "x", -1), take(left, "x", 1)
    f_left, f_right = take(m_left, "x", -1), take(p_right, "x", 1)
    return jnp.concatenate(
        [
            h,
            jnp.concatenate([m_left, m_right], axis=1),
            jnp.concatenate([f_left, f_right], axis=1),
            jnp.concatenate([p_left, p_right], axis=1),
        ],
        axis=0,
    )


def scatter_sum(parts):
    half = parts.shape[2] // 2
    narrow = parts.astype(BF)
    far_l = take(narrow[2][:, :half], "x", -1)
    far_r = take(narrow[2][:, half:], "x", 1)
    p_right = take(narrow[3][:, half:], "x", -1)
    m_left = take(narrow[1][:, :half], "x", 1)
    p_left = take((parts[3][:, :half] + far_l.astype(F32)).astype(BF), "x", -1)
    m_right = take((parts[1][:, half:] + far_r.astype(F32)).astype(BF), "x", 1)
    left = parts[0][:, :half] + p_left.astype(F32) + m_left.astype(F32)
    right = parts[0][:, half:] + p_right.astype(F32) + m_right.astype(F32)
    return jnp.concatenate([left, right], axis=1)


def sum_over_x(s):
    a, b, c = take(s, "x", -1), take(s, "x", 1), take(s, "x", 2)
    return s + jnp.roll(a, 1, axis=0) + jnp.roll(b, -1, axis=0) + jnp.roll(c, 2, axis=0)


def body(hidden, norm_gain, w_value, w_gate, conv_weight, conv_bias, chan_gain, chan_shift, w_out):
    z, y, x, c = (lax.axis_index(a) for a in SP_TP)
    own_rows, width = hidden.shape
    layers, rows, chans = w_value.shape
    taps = conv_weight.shape[1]
    keep = 32
    channels = chans * lax.axis_size("x") * lax.axis_size("c")
    z_cols = width // lax.axis_size("z")

    state = rolled(hidden, z * z_cols, 1)

    first = (z * lax.axis_size("y") + y) * rows
    weights = []
    for layer in range(layers):
        gain = lax.dynamic_slice_in_dim(norm_gain[layer], first, rows)[:, None]
        wv = (w_value[layer].astype(F32) * gain).astype(BF)
        wg = (w_gate[layer].astype(F32) * gain).astype(BF)
        wo = w_out[layer].T
        weights.append((jnp.concatenate([wv, wg], axis=1), wo))

    small = jnp.concatenate(
        [conv_weight, conv_bias[:, None], chan_gain[:, None], chan_shift[:, None]], axis=1
    )
    smalls = (small, swap(small))

    vg = gather_rows(weights[0][0])
    for layer in range(layers):
        xf = state.astype(F32)
        tokens = gather_tokens(state)
        tf = tokens.astype(F32)
        scale = lax.rsqrt(jnp.mean(tf * tf, axis=1, keepdims=True) + EPS)
        glus = []
        for half in range(2):
            both = jnp.dot(tokens, vg[half], preferred_element_type=F32)
            lin, gate = both[:, :chans] * scale, both[:, chans:] * scale
            glus.append((lin * jax.nn.sigmoid(gate)).astype(BF).reshape(4, own_rows, chans))
        if layer == 0:
            wo = gather_rows(weights[0][1])
        else:
            wo = (vg_wo[0][:, 2 * chans :], vg_wo[1][:, 2 * chans :])
        tails = jnp.concatenate([g[:, own_rows - keep :] for g in glus], axis=2)
        other = swap(tails)
        last = lax.dynamic_index_in_dim(tails, (x + 1) % 4, 0, keepdims=False)
        size = lax.axis_size("z") * lax.axis_size("y")
        pairs = [(2 * i + 1, 2 * (i + 1)) for i in range(size - 1)]
        before = lax.ppermute(last, ("z", "y", "c"), pairs)
        block = jnp.arange(4)[:, None, None]
        halo = jnp.where(
            c == 1, other, jnp.where(block == x, before[None], jnp.roll(other, -1, axis=0))
        )
        mixes, sums, squares = [], 0.0, 0.0
        for half in range(2):
            edge = halo[:, :, (1 - half) * chans : (2 - half) * chans]
            window = jnp.concatenate([edge, glus[half]], axis=1).astype(F32)
            par = smalls[half][layer]
            mixed = jnp.zeros((4, own_rows, chans), F32) + par[taps]
            for tap in range(taps):
                at = keep - (taps - 1) + tap
                mixed = mixed + par[tap] * window[:, at : at + own_rows]
            mixes.append(mixed)
            sums = sums + jnp.sum(mixed, axis=2)
            squares = squares + jnp.sum(mixed * mixed, axis=2)
        totals = sum_over_x(jnp.stack([sums, squares], axis=1))
        mean = (totals[:, 0] / channels)[:, :, None]
        msq = (totals[:, 1] / channels)[:, :, None]
        inv = lax.rsqrt(msq - mean * mean + EPS)
        partial = 0.0
        for half in range(2):
            par = smalls[half][layer]
            act = jax.nn.silu((mixes[half] - mean) * inv * par[taps + 1] + par[taps + 2]).astype(BF)
            act = act.reshape(4 * own_rows, chans)
            partial = partial + lax.dot_general(
                act, wo[half], (((1,), (1,)), ((), ())), preferred_element_type=F32
            )
        if layer == 0:
            vg_wo = gather_rows(jnp.concatenate(weights[1], axis=1))
            vg = (vg_wo[0][:, : 2 * chans], vg_wo[1][:, : 2 * chans])
        state = (xf + scatter_sum(partial.reshape(4, own_rows, width))).astype(BF)
    return rolled(state, ((8 - z) % 8) * z_cols, 1)


def solution(mesh):
    torus = Mesh(mesh.devices.reshape(8, 4, 4, 2), SP_TP)
    tp = ("x", "c")
    in_specs = (
        P(SP_TP, None),
        P(),
        P(None, SP, tp),
        P(None, SP, tp),
        P(None, None, tp),
        P(None, tp),
        P(None, tp),
        P(None, tp),
        P(None, tp, SP),
    )
    out_specs = P(SP_TP, None)
    return jax.shard_map(body, mesh=torus, in_specs=in_specs, out_specs=out_specs, check_vma=False)
```

```python
import functools

import jax
import jax.numpy as jnp
from jax import lax
from jax.experimental import pallas as pl
from jax.experimental.pallas import tpu as pltpu
from jax.sharding import Mesh
from jax.sharding import PartitionSpec as P

SP = ("z", "y")
SP_TP = ("z", "y", "x", "c")
EPS = 1e-06
BF = jnp.bfloat16
F32 = jnp.float32
ROWS = 96
CH = 256
TAPS = 31
KEEP = 32
WIDTH = 2048
CHANNELS = 2048


def take(a, axis, by):
    n = lax.axis_size(axis)
    return lax.ppermute(a, axis, [((i + by) % n, i) for i in range(n)])


def swap(a):
    return lax.ppermute(a, "c", [(0, 1), (1, 0)])


def rolled(a, start, axis):
    return lax.dynamic_slice_in_dim(jnp.concatenate([a, a], axis=axis), start, a.shape[axis], axis)


def after(a, *others):
    return lax.optimization_barrier((a, *others))[0]


def gather_y(a):
    y = lax.axis_index("y")
    near = jnp.concatenate([a, take(a, "y", 1), take(a, "y", 2), take(a, "y", 3)], axis=0)
    near = rolled(near, ((4 - y) % 4) * a.shape[0], 0)
    return jnp.concatenate([near[:, : 2 * CH], near[:, 2 * CH :].T], axis=1)


def gather_z(near, gates=((), (), (), ())):
    half = CH // 2
    a = after(near, *gates[0]) if gates[0] else near
    p1, m1 = take(a, "z", 1), take(a, "z", -1)
    b, c = (after(p1, *gates[1]), after(m1, *gates[1])) if gates[1] else (p1, m1)
    p2, m2 = take(b, "z", 1), take(c, "z", -1)
    s1 = swap(jnp.concatenate([near, p1, m1], axis=0))
    b, c = (after(p2, *gates[2]), after(m2, *gates[2])) if gates[2] else (p2, m2)
    p3, m3 = take(b, "z", 1), take(c, "z", -1)
    b, c = p3[:half], m3[half:]
    b, c = (after(b, *gates[3]), after(c, *gates[3])) if gates[3] else (b, c)
    far = jnp.concatenate([take(b, "z", 1), take(c, "z", -1)], axis=0)
    s2 = swap(jnp.concatenate([p2, m2, p3, m3], axis=0))
    s3 = swap(far)
    own = [(near, 0, 0), (p1, 0, 1), (m1, 0, 7), (p2, 0, 2), (m2, 0, 6), (p3, 0, 3), (m3, 0, 5), (far, 0, 4)]
    other = [(s1, 0, 0), (s1, 256, 1), (s1, 512, 7), (s2, 0, 2), (s2, 256, 6), (s2, 512, 3), (s2, 768, 5), (s3, 0, 4)]
    return own, other


def unique(chunks):
    arrays = []
    for a, _, _ in chunks:
        if not any(a is b for b in arrays):
            arrays.append(a)
    table = [(next(i for i, b in enumerate(arrays) if b is a), r, k) for a, r, k in chunks]
    return arrays, table


def gather_tokens(h):
    half = WIDTH // 2
    m, p = take(h, "x", -1), take(h, "x", 1)
    f_left, f_right = take(m[:, :half], "x", -1), take(p[:, half:], "x", 1)
    return h, m, f_left, f_right, p


def glu_kernel(*refs, n_own, n_other, tables):
    at_ref, own, m, f_left, f_right, p = refs[:6]
    w = (refs[6 : 6 + n_own], refs[6 + n_own : 6 + n_own + n_other])
    glu, tails, last, tok, acc = refs[6 + n_own + n_other :]
    half = WIDTH // 2
    tok[0:ROWS] = own[...]
    tok[ROWS : 2 * ROWS] = m[...]
    tok[2 * ROWS : 3 * ROWS, :half] = f_left[...]
    tok[2 * ROWS : 3 * ROWS, half:] = f_right[...]
    tok[3 * ROWS :] = p[...]
    total = jnp.zeros((4 * ROWS, 128), F32)
    for k in range(WIDTH // 128):
        t = tok[:, k * 128 : (k + 1) * 128].astype(F32)
        total = total + t * t
    scale = lax.rsqrt(jnp.sum(total, axis=1, keepdims=True) * (1.0 / WIDTH) + EPS)
    for s in range(2):
        for n, (i, r, k) in enumerate(tables[s]):
            d = jnp.dot(
                tok[:, k * CH : (k + 1) * CH], w[s][i][r : r + CH, : 2 * CH], preferred_element_type=F32
            )
            if n == 0:
                acc[...] = d
            else:
                acc[...] += d
        lin, gate = acc[:, :CH] * scale, acc[:, CH:] * scale
        glu[:, s * CH : (s + 1) * CH] = (lin / (1.0 + jnp.exp(-gate))).astype(BF)
    for r in range(4):
        tails[r * KEEP : (r + 1) * KEEP] = glu[(r + 1) * ROWS - KEEP : (r + 1) * ROWS]
    last[...] = tails[pl.ds(pl.multiple_of(((at_ref[0] + 1) % 4) * KEEP, KEEP), KEEP)]


def whole(n):
    return [pl.BlockSpec(memory_space=pltpu.VMEM)] * n


def call(kernel, outs, inputs, scratch=(), scalars=True):
    n = len(inputs) - (1 if scalars else 0)
    specs = ([pl.BlockSpec(memory_space=pltpu.SMEM)] if scalars else []) + whole(n)
    return pl.pallas_call(
        kernel,
        out_shape=[jax.ShapeDtypeStruct(s, d) for s, d in outs],
        in_specs=specs,
        out_specs=whole(len(outs)),
        scratch_shapes=list(scratch),
        compiler_params=pltpu.CompilerParams(vmem_limit_bytes=48 * 1024 * 1024),
    )(*inputs)


def glu_call(at, tokens, own, other):
    a, ta = unique(own)
    b, tb = unique(other)
    return call(
        functools.partial(glu_kernel, n_own=len(a), n_other=len(b), tables=(ta, tb)),
        [((4 * ROWS, 2 * CH), BF), ((4 * KEEP, 2 * CH), BF), ((KEEP, 2 * CH), BF)],
        [at, *tokens, *a, *b],
        [pltpu.VMEM((4 * ROWS, WIDTH), BF), pltpu.VMEM((4 * ROWS, 2 * CH), F32)],
    )


def conv_kernel(at_ref, glu, other, before, par_a, par_b, mixed, stats, win):
    x, c = at_ref[0], at_ref[1]
    stats[...] = jnp.zeros((8, 128), F32)

    def block(r, _):
        idx = jnp.where(c == 1, r, (r + 1) % 4)
        first = jnp.logical_and(c == 0, r == x)
        at = pl.multiple_of(r * ROWS, ROWS)
        edge_at = pl.multiple_of(idx * KEEP, KEEP)
        s1 = jnp.zeros((ROWS, 128), F32)
        s2 = jnp.zeros((ROWS, 128), F32)
        for strip in range(4):
            lanes = slice(strip * 128, (strip + 1) * 128)
            there = slice(((strip + 2) % 4) * 128, ((strip + 2) % 4) * 128 + 128)
            edge = jnp.where(first, before[:, there].astype(F32), other[pl.ds(edge_at, KEEP), there].astype(F32))
            win[0:KEEP] = edge
            win[KEEP:] = glu[pl.ds(at, ROWS), lanes].astype(F32)
            par = par_a if strip < 2 else par_b
            pl_ = slice((strip % 2) * 128, (strip % 2) * 128 + 128)
            acc = jnp.zeros((ROWS, 128), F32) + par[TAPS : TAPS + 1, pl_]
            for s in range(8):
                shifted = win[s : s + (120 if s else 128)]
                for base in range(0, 40, 8):
                    tap = base + s - (KEEP - (TAPS - 1))
                    if 0 <= tap < TAPS:
                        acc = acc + par[tap : tap + 1, pl_] * shifted[base : base + ROWS]
            mixed[pl.ds(at, ROWS), lanes] = acc
            s1 = s1 + acc
            s2 = s2 + acc * acc
        stats[pl.ds(r, 1), 0:ROWS] = jnp.sum(s1.T, axis=0, keepdims=True)
        stats[pl.ds(r + 4, 1), 0:ROWS] = jnp.sum(s2.T, axis=0, keepdims=True)
        return 0

    lax.fori_loop(0, 4, block, 0)


def conv_call(at, glu, other, before, par_a, par_b):
    return call(
        conv_kernel,
        [((4 * ROWS, 2 * CH), F32), ((8, 128), F32)],
        [at, glu, other, before, par_a, par_b],
        [pltpu.VMEM((KEEP + ROWS, 128), F32)],
    )


def out_kernel(*refs, n_own, n_other, tables):
    mixed, s0, sm, sp, sf, par_a, par_b = refs[:7]
    w = (refs[7 : 7 + n_own], refs[7 + n_own : 7 + n_own + n_other])
    out0, out1, out2, out3, act = refs[7 + n_own + n_other :]
    rows = []
    for q in range(2):
        for r in range(4):
            o = 4 * q
            rows.append(
                s0[o + r : o + r + 1]
                + sm[o + (r - 1) % 4 : o + (r - 1) % 4 + 1]
                + sp[o + (r + 1) % 4 : o + (r + 1) % 4 + 1]
                + sf[o + (r + 2) % 4 : o + (r + 2) % 4 + 1]
            )
    mean = jnp.concatenate(rows[:4], axis=0) * (1.0 / CHANNELS)
    msq = jnp.concatenate(rows[4:], axis=0) * (1.0 / CHANNELS)
    inv = lax.rsqrt(msq - mean * mean + EPS)
    cols = jnp.concatenate([mean, inv], axis=0).T
    for r in range(4):
        mu, iv = cols[:ROWS, r : r + 1], cols[:ROWS, 4 + r : 5 + r]
        for s, par in ((0, par_a), (1, par_b)):
            v = (mixed[r * ROWS : (r + 1) * ROWS, s * CH : (s + 1) * CH] - mu) * iv
            v = v * par[TAPS + 1 : TAPS + 2] + par[TAPS + 2 : TAPS + 3]
            act[r * ROWS : (r + 1) * ROWS, s * CH : (s + 1) * CH] = (v / (1.0 + jnp.exp(-v))).astype(BF)
    where = [{k: (i, r) for i, r, k in t} for t in tables]
    for k in range(WIDTH // CH):
        (i, r), (j, q) = where[0][k], where[1][k]
        d = jnp.dot(act[:, :CH], w[0][i][r : r + CH, 2 * CH :], preferred_element_type=F32)
        d = d + jnp.dot(act[:, CH:], w[1][j][q : q + CH, 2 * CH :], preferred_element_type=F32)
        cols_k = slice(k * CH, (k + 1) * CH)
        out0[:, cols_k] = d[:ROWS]
        out1[:, cols_k] = d[ROWS : 2 * ROWS].astype(BF)
        out2[:, cols_k] = d[2 * ROWS : 3 * ROWS].astype(BF)
        out3[:, cols_k] = d[3 * ROWS :].astype(BF)


def out_call(mixed, stats, par_a, par_b, own, other):
    a, ta = unique(own)
    b, tb = unique(other)
    return call(
        functools.partial(out_kernel, n_own=len(a), n_other=len(b), tables=(ta, tb)),
        [((ROWS, WIDTH), F32)] + [((ROWS, WIDTH), BF)] * 3,
        [mixed, *stats, par_a, par_b, *a, *b],
        [pltpu.VMEM((4 * ROWS, 2 * CH), BF)],
        scalars=False,
    )


def body(hidden, norm_gain, w_value, w_gate, conv_weight, conv_bias, chan_gain, chan_shift, w_out):
    z, y, x, c = (lax.axis_index(a) for a in SP_TP)
    layers, rows, _ = w_value.shape
    z_cols = WIDTH // lax.axis_size("z")
    at = jnp.stack([x, c]).astype(jnp.int32)

    first = (z * lax.axis_size("y") + y) * rows
    bundles = []
    for layer in range(layers):
        gain = lax.dynamic_slice_in_dim(norm_gain[layer], first, rows)[:, None]
        wv = (w_value[layer].astype(F32) * gain).astype(BF)
        wg = (w_gate[layer].astype(F32) * gain).astype(BF)
        bundles.append(jnp.concatenate([wv, wg, w_out[layer].T], axis=1))
    small = jnp.concatenate(
        [conv_weight, conv_bias[:, None], chan_gain[:, None], chan_shift[:, None]], axis=1
    )

    near = gather_y(bundles[0])
    chunks = gather_z(near)
    state = rolled(hidden, z * z_cols, 1)
    near_next = gather_y(after(bundles[1], near))
    smalls = (small, swap(after(small, near)))
    half = WIDTH // 2
    for layer in range(layers):
        tokens = gather_tokens(state)
        par_a, par_b = smalls[0][layer], smalls[1][layer]
        glu, tails, last = glu_call(at, tokens, *chunks)
        other = swap(tails)
        size = lax.axis_size("z") * lax.axis_size("y")
        pairs = [(2 * i + 1, 2 * (i + 1)) for i in range(size - 1)]
        before = lax.ppermute(last, ("z", "y", "c"), pairs)
        mixed, s = conv_call(at, glu, other, before, par_a, par_b)
        stats = (s, take(s, "x", -1), take(s, "x", 1), take(s, "x", 2))
        o0, o1, o2, o3 = out_call(mixed, stats, par_a, par_b, *chunks)
        if layer == 0:
            chunks = gather_z(near_next, ((glu,), (mixed,), (o2,), (o2,)))
        far_l, far_r = take(o2[:, :half], "x", -1), take(o2[:, half:], "x", 1)
        to_p = jnp.concatenate([o3[:, :half] + far_l, o3[:, half:]], axis=1)
        to_m = jnp.concatenate([o1[:, :half], o1[:, half:] + far_r], axis=1)
        from_m, from_p = take(to_p, "x", -1), take(to_m, "x", 1)
        total = state.astype(F32) + (o0 + from_m.astype(F32) + from_p.astype(F32))
        state = total.astype(BF)
    return rolled(state, ((8 - z) % 8) * z_cols, 1)


def solution(mesh):
    torus = Mesh(mesh.devices.reshape(8, 4, 4, 2), SP_TP)
    tp = ("x", "c")
    in_specs = (
        P(SP_TP, None),
        P(),
        P(None, SP, tp),
        P(None, SP, tp),
        P(None, None, tp),
        P(None, tp),
        P(None, tp),
        P(None, tp),
        P(None, tp, SP),
    )
    out_specs = P(SP_TP, None)
    return jax.shard_map(body, mesh=torus, in_specs=in_specs, out_specs=out_specs, check_vma=False)
```

```python
import functools

import jax
import jax.numpy as jnp
from jax import lax
from jax.experimental import pallas as pl
from jax.experimental.pallas import tpu as pltpu
from jax.sharding import Mesh
from jax.sharding import PartitionSpec as P


SP = ("z", "y")
SP_TP = ("z", "y", "x", "c")
EPS = 1e-06
BF = jnp.bfloat16
F32 = jnp.float32
ROWS = 96
CH = 256
TAPS = 31
KEEP = 32
REST = ROWS - KEEP
WIDTH = 2048
CHANNELS = 2048
BUNDLE = 3 * CH
PIECE = 64


def take(a, axis, by):
    n = lax.axis_size(axis)
    return lax.ppermute(a, axis, [((i + by) % n, i) for i in range(n)])


def swap(a):
    return lax.ppermute(a, "c", [(0, 1), (1, 0)])


def rolled(a, start, axis):
    return lax.dynamic_slice_in_dim(jnp.concatenate([a, a], axis=axis), start, a.shape[axis], axis)


def call(kernel, outs, inputs, scratch=(), scalars=True):
    n = len(inputs) - (1 if scalars else 0)
    vmem = pl.BlockSpec(memory_space=pltpu.VMEM)
    specs = ([pl.BlockSpec(memory_space=pltpu.SMEM)] if scalars else []) + [vmem] * n
    return pl.pallas_call(
        kernel,
        out_shape=[jax.ShapeDtypeStruct(s, d) for s, d in outs],
        in_specs=specs,
        out_specs=[vmem] * len(outs),
        scratch_shapes=list(scratch),
        compiler_params=pltpu.CompilerParams(vmem_limit_bytes=32 * 1024 * 1024),
    )(*inputs)


def first_kernel(at, hidden, gain, wv, wg, wo, cw, cb, cg, cs, b0, b1, state, par, col):
    z = at[0]
    sp = z * 4 + at[1]
    for layer, out in ((0, b0), (1, b1)):
        lane = pl.multiple_of((sp // 2) * 128, 128)
        g = gain[layer : layer + 1, pl.ds(lane, 128)]
        col[...] = jnp.broadcast_to(g, (128, 128)).T
        g = col[pl.ds(pl.multiple_of((sp % 2) * PIECE, PIECE), PIECE), 0:1]
        out[:, :CH] = (wv[layer].astype(F32) * g).astype(BF)
        out[:, CH : 2 * CH] = (wg[layer].astype(F32) * g).astype(BF)
        out[:, 2 * CH :] = wo[layer]
    for layer in range(2):
        par[layer, :TAPS] = cw[layer]
        for n, a in enumerate((cb, cg, cs)):
            par[layer, TAPS + n : TAPS + n + 1] = a[layer : layer + 1]
    for k in range(8):
        src = pl.multiple_of(((z + k) % 8) * CH, CH)
        state[:, k * CH : (k + 1) * CH] = hidden[:, pl.ds(src, CH)]


def near_kernel(at, a0, a1, a2, a3, out):
    y = at[1]
    for k, a in enumerate((a0, a1, a2, a3)):
        out[pl.ds(pl.multiple_of(((y + k) % 4) * PIECE, PIECE), PIECE)] = a[...]


def spread(at, refs, table, dst, lanes, out_lanes):
    for i, r, place, n in table:
        base, step = place, PIECE
        if isinstance(place, tuple):
            base, step = ((at[1] + place[0]) % 4) * PIECE, CH

        def piece(j, _, i=i, r=r, base=base, step=step):
            src = pl.multiple_of(r + j * PIECE, PIECE)
            to = pl.multiple_of(base + j * step, PIECE)
            dst[pl.ds(to, PIECE), out_lanes] = refs[i][pl.ds(src, PIECE), lanes]
            return 0

        lax.fori_loop(0, n // PIECE, piece, 0)


def glu_first_kernel(*refs, n, table):
    at, own, m, f, p = refs[:5]
    w = refs[5 : 5 + n]
    glu, tok, scale, full = refs[5 + n :]
    for r, a in enumerate((own, m, f, p)):
        tok[r * ROWS : (r + 1) * ROWS] = a[...]
        t = jnp.zeros((ROWS, 128), F32)
        for k in range(WIDTH // 128):
            v = a[:, k * 128 : (k + 1) * 128].astype(F32)
            t = t + v * v
        s = lax.rsqrt(jnp.sum(t, axis=1, keepdims=True) * (1.0 / WIDTH) + EPS)
        scale[r * ROWS : (r + 1) * ROWS] = jnp.broadcast_to(s, (ROWS, 128))
    spread(at, w, table, full, slice(0, 2 * CH), slice(0, 2 * CH))
    both = jnp.dot(tok[...], full[...], preferred_element_type=F32)
    s = scale[:, 0:1]
    lin, gate = both[:, :CH] * s, both[:, CH:] * s
    glu[...] = (lin / (1.0 + jnp.exp(-gate))).astype(BF)


def glu_second_kernel(*refs, n, table):
    at, tok, scale, other = refs[:4]
    w = refs[4 : 4 + n]
    glu, tails, last, full = refs[4 + n :]
    spread(at, w, table, full, slice(0, 2 * CH), slice(0, 2 * CH))
    both = jnp.dot(tok[...], full[...], preferred_element_type=F32)
    s = scale[:, 0:1]
    lin, gate = both[:, :CH] * s, both[:, CH:] * s
    glu[...] = (lin / (1.0 + jnp.exp(-gate))).astype(BF)
    for r in range(4):
        here = slice((r + 1) * ROWS - KEEP, (r + 1) * ROWS)
        tails[r * KEEP : (r + 1) * KEEP, :CH] = other[here]
        tails[r * KEEP : (r + 1) * KEEP, CH:] = glu[here]
    last[...] = tails[pl.ds(pl.multiple_of(((at[2] + 1) % 4) * KEEP, KEEP), KEEP)]


def glu_calls(at, tokens, own, other):
    (a, ta), (b, tb) = own, other
    size = (4 * ROWS, CH)
    full = pltpu.VMEM((WIDTH, 2 * CH), BF)
    glu_a, tok, scale = call(
        functools.partial(glu_first_kernel, n=len(a), table=ta),
        [(size, BF), ((4 * ROWS, WIDTH), BF), ((4 * ROWS, 128), F32)],
        [at, *tokens, *a],
        [full],
    )
    glu_b, tails, last = call(
        functools.partial(glu_second_kernel, n=len(b), table=tb),
        [(size, BF), ((4 * KEEP, 2 * CH), BF), ((KEEP, 2 * CH), BF)],
        [at, tok, scale, glu_a, *b],
        [full],
    )
    return glu_a, glu_b, tails, last


def conv_strip(win, par, lanes, rows):
    acc = jnp.zeros((rows, 128), F32) + par[TAPS : TAPS + 1, lanes]
    for s in range(8):
        shifted = win[s : s + rows + (24 if s else 32)]
        for base in range(0, 40, 8):
            tap = base + s - (KEEP - (TAPS - 1))
            if 0 <= tap < TAPS:
                acc = acc + par[tap : tap + 1, lanes] * shifted[base : base + rows]
    return acc


def row_of(sums, lead):
    parts = [sums]
    if lead:
        parts = [jnp.zeros((lead, 128), F32)] + parts
    missing = 128 - lead - sums.shape[0]
    parts.append(jnp.zeros((missing, 128), F32))
    return jnp.sum(jnp.concatenate(parts, axis=0).T, axis=0, keepdims=True)


def conv_rest_kernel(*refs, n, m, tables, layer):
    at, glu_a, glu_b = refs[:3]
    par_a, par_b = refs[3].at[layer], refs[4].at[layer]
    wa, wb = refs[5 : 5 + n], refs[5 + n : 5 + n + m]
    mixed, stats, wo, win = refs[5 + n + m :]

    def block(r, _):
        here = pl.multiple_of(r * ROWS, KEEP)
        s1 = jnp.zeros((REST, 128), F32)
        s2 = jnp.zeros((REST, 128), F32)
        for strip in range(4):
            lanes = slice((strip % 2) * 128, (strip % 2) * 128 + 128)
            glu, par = (glu_a, par_a) if strip < 2 else (glu_b, par_b)
            win[...] = glu[pl.ds(here, ROWS), lanes].astype(F32)
            acc = conv_strip(win, par, lanes, REST)
            mixed[pl.ds(pl.multiple_of(r * REST, REST), REST), strip * 128 : strip * 128 + 128] = acc
            s1 = s1 + acc
            s2 = s2 + acc * acc
        stats[pl.ds(r, 1)] = row_of(s1, KEEP)
        stats[pl.ds(r + 4, 1)] = row_of(s2, KEEP)
        return 0

    lax.fori_loop(0, 4, block, 0)
    spread(at, wa, tables[0], wo, slice(2 * CH, 3 * CH), slice(0, CH))
    spread(at, wb, tables[1], wo, slice(2 * CH, 3 * CH), slice(CH, 2 * CH))


def conv_edge_kernel(at, glu_a, glu_b, other, before, par_a, par_b, stats_in, mixed, stats, win, *, layer):
    par_a, par_b = par_a.at[layer], par_b.at[layer]
    x, c = at[2], at[3]

    def block(r, _):
        idx = jnp.where(c == 1, r, (r + 1) % 4)
        first = jnp.logical_and(c == 0, r == x)
        here = pl.multiple_of(r * ROWS, KEEP)
        edge_at = pl.multiple_of(idx * KEEP, KEEP)
        s1 = jnp.zeros((KEEP, 128), F32)
        s2 = jnp.zeros((KEEP, 128), F32)
        for strip in range(4):
            lanes = slice((strip % 2) * 128, (strip % 2) * 128 + 128)
            there = slice(((strip + 2) % 4) * 128, ((strip + 2) % 4) * 128 + 128)
            glu, par = (glu_a, par_a) if strip < 2 else (glu_b, par_b)
            edge = other[pl.ds(edge_at, KEEP), there].astype(F32)
            win[0:KEEP] = jnp.where(first, before[:, there].astype(F32), edge)
            win[KEEP:] = glu[pl.ds(here, KEEP), lanes].astype(F32)
            acc = conv_strip(win, par, lanes, KEEP)
            mixed[pl.ds(pl.multiple_of(r * KEEP, KEEP), KEEP), strip * 128 : strip * 128 + 128] = acc
            s1 = s1 + acc
            s2 = s2 + acc * acc
        stats[pl.ds(r, 1)] = stats_in[pl.ds(r, 1)] + row_of(s1, 0)
        stats[pl.ds(r + 4, 1)] = stats_in[pl.ds(r + 4, 1)] + row_of(s2, 0)
        return 0

    lax.fori_loop(0, 4, block, 0)


def out_kernel(*refs, blocks, layer):
    at, low, high, stats, par_a, par_b, wo = refs[:7]
    outs, act = refs[7:-1], refs[-1]
    par_a, par_b = par_a.at[layer], par_b.at[layer]
    x = at[2]
    own, m, f, p = (stats[pl.ds(pl.multiple_of(((x + d) % 4) * 8, 8), 8)] for d in (0, 3, 2, 1))
    rows = []
    for o in (0, 4):
        for r in range(4):
            i, j, k = o + (r - 1) % 4, o + (r + 2) % 4, o + (r + 1) % 4
            rows.append(own[o + r : o + r + 1] + m[i : i + 1] + f[j : j + 1] + p[k : k + 1])
    mean = jnp.concatenate(rows[:4], axis=0) * (1.0 / CHANNELS)
    msq = jnp.concatenate(rows[4:], axis=0) * (1.0 / CHANNELS)
    inv = lax.rsqrt(msq - mean * mean + EPS)
    cols = jnp.concatenate([mean, inv], axis=0).T
    for n, r in enumerate(blocks):
        for src, size, first in ((low, KEEP, 0), (high, REST, KEEP)):
            mu = cols[first : first + size, r : r + 1]
            iv = cols[first : first + size, 4 + r : 5 + r]
            for s, par in ((0, par_a), (1, par_b)):
                v = (src[r * size : (r + 1) * size, s * CH : (s + 1) * CH] - mu) * iv
                v = v * par[TAPS + 1 : TAPS + 2] + par[TAPS + 2 : TAPS + 3]
                to = n * ROWS + first
                act[to : to + size, s * CH : (s + 1) * CH] = (v / (1.0 + jnp.exp(-v))).astype(BF)
    d = lax.dot_general(act[...], wo[...], (((1,), (1,)), ((), ())), preferred_element_type=F32)
    for n, out in enumerate(outs):
        out[...] = d[n * ROWS : (n + 1) * ROWS].astype(out.dtype)


def out_call(layer, blocks, kinds, *inputs):
    return call(
        functools.partial(out_kernel, blocks=blocks, layer=layer),
        [((ROWS, WIDTH), k) for k in kinds],
        list(inputs),
        [pltpu.VMEM((len(blocks) * ROWS, 2 * CH), BF)],
    )


def layer_body(layer, at, state, tokens, own, other, par, before_pairs):
    glu_a, glu_b, tails, last = glu_calls(at, tokens, own, other)
    there = swap(tails)
    before = lax.ppermute(last, ("z", "y", "c"), before_pairs)
    par_a, par_b = par
    (a, ta), (b, tb) = own, other
    high, part, wo = call(
        functools.partial(conv_rest_kernel, n=len(a), m=len(b), tables=(ta, tb), layer=layer),
        [((4 * REST, 2 * CH), F32), ((8, 128), F32), ((WIDTH, 2 * CH), BF)],
        [at, glu_a, glu_b, par_a, par_b, *a, *b],
        [pltpu.VMEM((ROWS, 128), F32)],
    )
    low, s = call(
        functools.partial(conv_edge_kernel, layer=layer),
        [((4 * KEEP, 2 * CH), F32), ((8, 128), F32)],
        [at, glu_a, glu_b, there, before, par_a, par_b, part],
        [pltpu.VMEM((2 * KEEP, 128), F32)],
    )
    stats = lax.all_to_all(jnp.broadcast_to(s[None], (4, 8, 128)), "x", 0, 0, tiled=True)
    inputs = (at, low, high, stats.reshape(32, 128), par_a, par_b, wo)
    (o2,) = out_call(layer, (2,), (BF,), *inputs)
    from_f = take(o2, "x", 2)
    o3, o1, o0 = out_call(layer, (3, 1, 0), (BF, BF, F32), *inputs)
    from_m, from_p = take(o3, "x", -1), take(o1, "x", 1)
    total = o0 + from_m.astype(F32) + from_p.astype(F32) + from_f.astype(F32)
    return (state.astype(F32) + total).astype(BF)


def gather_tokens(h):
    m, p, f = take(h, "x", -1), take(h, "x", 1), take(h, "x", 2)
    return h, m, f, p


def body(hidden, norm_gain, w_value, w_gate, conv_weight, conv_bias, chan_gain, chan_shift, w_out):
    z, y, x, c = (lax.axis_index(a) for a in SP_TP)
    at = jnp.stack([z, y, x, c]).astype(jnp.int32)
    half = CH // 2
    b0, b1, state, small = call(
        first_kernel,
        [((PIECE, BUNDLE), BF), ((PIECE, BUNDLE), BF), ((ROWS, WIDTH), BF), ((2, 40, CH), F32)],
        [at, hidden, norm_gain, w_value, w_gate, w_out.swapaxes(1, 2)]
        + [conv_weight, conv_bias, chan_gain, chan_shift],
        [pltpu.VMEM((128, 128), F32)],
    )
    g = [b0, take(b0, "y", 1), take(b0, "y", 2), take(b0, "y", 3)]
    (near,) = call(near_kernel, [((CH, BUNDLE), BF)], [at, *g])
    p1, m1 = take(near, "z", 1), take(near, "z", -1)
    p2, m2 = take(p1, "z", 1), take(m1, "z", -1)
    s1 = swap(jnp.concatenate([near, p1, m1], axis=0))
    p3, m3 = take(p2, "z", 1), take(m2, "z", -1)
    top, low = take(p3[:half], "z", 1), take(m3[half:], "z", -1)
    s2 = swap(jnp.concatenate([p2, m2, p3, m3], axis=0))
    s3 = swap(jnp.concatenate([top, low], axis=0))
    own0 = (
        [near, p1, m1, p2, m2, p3, m3, top, low],
        [(i, 0, k * CH, CH) for i, k in enumerate((0, 1, 7, 2, 6, 3, 5))]
        + [(7, 0, 4 * CH, half), (8, 0, 4 * CH + half, half)],
    )
    other0 = (
        [s1, s2, s3],
        [(0, i * CH, k * CH, CH) for i, k in enumerate((0, 1, 7))]
        + [(1, i * CH, k * CH, CH) for i, k in enumerate((2, 6, 3, 5))]
        + [(2, 0, 4 * CH, CH)],
    )

    za, zb, z4 = take(b1, "z", 1), take(b1, "z", -1), take(b1, "z", 4)
    z2 = take(jnp.concatenate([b1, za], axis=0), "z", 2)
    z6 = take(jnp.concatenate([b1, zb], axis=0), "z", -2)
    line = jnp.concatenate([b1, za, z2, z4, z6[PIECE:], z6[:PIECE], zb], axis=0)
    up, down = take(line, "y", 1), take(line, "y", -1)
    across = take(line, "y", 2)
    ysw = swap(jnp.concatenate([line, up, down, across], axis=0))
    size = 8 * PIECE
    own1 = (
        [line, up, down, across],
        [(0, 0, (0,), size), (1, 0, (1,), size), (2, 0, (3,), size), (3, 0, (2,), size)],
    )
    other1 = (
        [ysw],
        [(0, n * size, (dy,), size) for n, dy in enumerate((0, 1, 3, 2))],
    )
    par = (small, swap(small))
    size = lax.axis_size("z") * lax.axis_size("y")
    pairs = [(2 * i + 1, 2 * (i + 1)) for i in range(size - 1)]
    state = layer_body(0, at, state, gather_tokens(state), own0, other0, par, pairs)
    state = layer_body(1, at, state, gather_tokens(state), own1, other1, par, pairs)
    return rolled(state, ((8 - z) % 8) * (WIDTH // 8), 1)


def solution(mesh):
    torus = Mesh(mesh.devices.reshape(8, 4, 4, 2), SP_TP)
    tp = ("x", "c")
    in_specs = (
        P(SP_TP, None),
        P(),
        P(None, SP, tp),
        P(None, SP, tp),
        P(None, None, tp),
        P(None, tp),
        P(None, tp),
        P(None, tp),
        P(None, tp, SP),
    )
    return jax.shard_map(
        body, mesh=torus, in_specs=in_specs, out_specs=P(SP_TP, None), check_vma=False
    )
```

```python
import functools

import jax
import jax.numpy as jnp
from jax import lax
from jax.experimental import pallas as pl
from jax.experimental.pallas import tpu as pltpu
from jax.sharding import Mesh
from jax.sharding import PartitionSpec as P


SP = ("z", "y")
SP_TP = ("z", "y", "x", "c")
EPS = 1e-06
BF = jnp.bfloat16
F32 = jnp.float32
ROWS = 96
CH = 256
TAPS = 31
KEEP = 32
REST = ROWS - KEEP
WIDTH = 2048
CHANNELS = 2048
BUNDLE = 3 * CH
PIECE = 64


def take(a, axis, by):
    n = lax.axis_size(axis)
    return lax.ppermute(a, axis, [((i + by) % n, i) for i in range(n)])


def swap(a):
    return lax.ppermute(a, "c", [(0, 1), (1, 0)])


def call(kernel, outs, inputs, scratch=(), scalars=True):
    n = len(inputs) - (1 if scalars else 0)
    vmem = pl.BlockSpec(memory_space=pltpu.VMEM)
    specs = ([pl.BlockSpec(memory_space=pltpu.SMEM)] if scalars else []) + [vmem] * n
    return pl.pallas_call(
        kernel,
        out_shape=[jax.ShapeDtypeStruct(s, d) for s, d in outs],
        in_specs=specs,
        out_specs=[vmem] * len(outs),
        scratch_shapes=list(scratch),
        compiler_params=pltpu.CompilerParams(vmem_limit_bytes=12 * 1024 * 1024),
    )(*inputs)


def fold_kernel(at, gain, wv, wg, wo, b0, b1, col):
    sp = at[0] * 4 + at[1]
    for layer, out in ((0, b0), (1, b1)):
        lane = pl.multiple_of((sp // 2) * 128, 128)
        g = gain[layer : layer + 1, pl.ds(lane, 128)]
        col[...] = jnp.broadcast_to(g, (128, 128)).T
        g = col[pl.ds(pl.multiple_of((sp % 2) * PIECE, PIECE), PIECE), 0:1]
        out[:, :CH] = (wv[layer].astype(F32) * g).astype(BF)
        out[:, CH : 2 * CH] = (wg[layer].astype(F32) * g).astype(BF)
        out[:, 2 * CH :] = wo[layer]


def roll_kernel(at, hidden, state):
    for k in range(8):
        src = pl.multiple_of(((at[0] + k) % 8) * CH, CH)
        state[:, k * CH : (k + 1) * CH] = hidden[:, pl.ds(src, CH)]


def par_kernel(cw, cb, cg, cs, par):
    for layer in range(2):
        par[layer, :TAPS] = cw[:, layer]
        for n, a in enumerate((cb, cg, cs)):
            par[layer, TAPS + n : TAPS + n + 1] = a[layer : layer + 1]


def near_kernel(at, a0, a1, a2, a3, out):
    y = at[1]
    for k, a in enumerate((a0, a1, a2, a3)):
        out[pl.ds(pl.multiple_of(((y + k) % 4) * PIECE, PIECE), PIECE)] = a[...]


def line_kernel(own, za, zb, z2, z4, z6, out):
    pieces = (own, za, z2.at[:PIECE], z2.at[PIECE:], z4, z6.at[PIECE:], z6.at[:PIECE], zb)
    for k, a in enumerate(pieces):
        out[k * PIECE : (k + 1) * PIECE] = a[...]


def cat_kernel(*refs):
    out = refs[-1]
    for k, a in enumerate(refs[:8]):
        out[k * CH : (k + 1) * CH] = a[...]


def spread(at, refs, table, dst, lanes, out_lanes):
    for i, r, place, n in table:
        base, step = place, PIECE
        if isinstance(place, tuple):
            base, step = place[1] * CH + ((at[1] + place[0]) % 4) * PIECE, CH

        def piece(j, _, i=i, r=r, base=base, step=step):
            src = pl.multiple_of(r + j * PIECE, PIECE)
            to = pl.multiple_of(base + j * step, PIECE)
            dst[pl.ds(to, PIECE), out_lanes] = refs[i][pl.ds(src, PIECE), lanes]
            return 0

        lax.fori_loop(0, n // PIECE, piece, 0)


def glu_first_kernel(*refs, n, table):
    at, own, m, f, p = refs[:5]
    w = refs[5 : 5 + n]
    glu, tok, scale, full = refs[5 + n :]
    for r, a in enumerate((own, m, f, p)):
        tok[r * ROWS : (r + 1) * ROWS] = a[...]
        t = jnp.zeros((ROWS, 128), F32)
        for k in range(WIDTH // 128):
            v = a[:, k * 128 : (k + 1) * 128].astype(F32)
            t = t + v * v
        s = lax.rsqrt(jnp.sum(t, axis=1, keepdims=True) * (1.0 / WIDTH) + EPS)
        scale[r * ROWS : (r + 1) * ROWS] = jnp.broadcast_to(s, (ROWS, 128))
    spread(at, w, table, full, slice(0, 2 * CH), slice(0, 2 * CH))
    both = jnp.dot(tok[...], full[...], preferred_element_type=F32)
    s = scale[:, 0:1]
    lin, gate = both[:, :CH] * s, both[:, CH:] * s
    glu[...] = (lin / (1.0 + jnp.exp(-gate))).astype(BF)


def glu_second_kernel(*refs, n, table):
    at, tok, scale, other = refs[:4]
    w = refs[4 : 4 + n]
    glu, tails, last, full = refs[4 + n :]
    spread(at, w, table, full, slice(0, 2 * CH), slice(0, 2 * CH))
    both = jnp.dot(tok[...], full[...], preferred_element_type=F32)
    s = scale[:, 0:1]
    lin, gate = both[:, :CH] * s, both[:, CH:] * s
    glu[...] = (lin / (1.0 + jnp.exp(-gate))).astype(BF)
    for r in range(4):
        here = slice((r + 1) * ROWS - KEEP, (r + 1) * ROWS)
        tails[r * KEEP : (r + 1) * KEEP, :CH] = other[here]
        tails[r * KEEP : (r + 1) * KEEP, CH:] = glu[here]
    last[...] = tails[pl.ds(pl.multiple_of(((at[2] + 1) % 4) * KEEP, KEEP), KEEP)]


def glu_calls(at, tokens, own, other):
    (a, ta), (b, tb) = own, other
    size = (4 * ROWS, CH)
    full = pltpu.VMEM((WIDTH, 2 * CH), BF)
    glu_a, tok, scale = call(
        functools.partial(glu_first_kernel, n=len(a), table=ta),
        [(size, BF), ((4 * ROWS, WIDTH), BF), ((4 * ROWS, 128), F32)],
        [at, *tokens, *a],
        [full],
    )
    glu_b, tails, last = call(
        functools.partial(glu_second_kernel, n=len(b), table=tb),
        [(size, BF), ((4 * KEEP, 2 * CH), BF), ((KEEP, 2 * CH), BF)],
        [at, tok, scale, glu_a, *b],
        [full],
    )
    return glu_a, glu_b, tails, last


def conv_strip(win, par, lanes, rows):
    acc = jnp.zeros((rows, 128), F32) + par[TAPS : TAPS + 1, lanes]
    for s in range(8):
        shifted = win[s : s + rows + (24 if s else 32)]
        for base in range(0, 40, 8):
            tap = base + s - (KEEP - (TAPS - 1))
            if 0 <= tap < TAPS:
                acc = acc + par[tap : tap + 1, lanes] * shifted[base : base + rows]
    return acc


def conv_rest_kernel(*refs, n, m, tables, layer):
    at, glu_a, glu_b = refs[:3]
    par_a, par_b = refs[3].at[layer], refs[4].at[layer]
    wa, wb = refs[5 : 5 + n], refs[5 + n : 5 + n + m]
    mixed, t1, t2, wo, win = refs[5 + n + m :]

    def block(r, _):
        here = pl.multiple_of(r * ROWS, KEEP)
        s1 = jnp.zeros((REST, 128), F32)
        s2 = jnp.zeros((REST, 128), F32)
        for strip in range(4):
            lanes = slice((strip % 2) * 128, (strip % 2) * 128 + 128)
            glu, par = (glu_a, par_a) if strip < 2 else (glu_b, par_b)
            win[...] = glu[pl.ds(here, ROWS), lanes].astype(F32)
            acc = conv_strip(win, par, lanes, REST)
            mixed[pl.ds(pl.multiple_of(r * REST, REST), REST), strip * 128 : strip * 128 + 128] = acc
            s1 = s1 + acc
            s2 = s2 + acc * acc
        t1[pl.ds(pl.multiple_of(r * REST, REST), REST)] = s1
        t2[pl.ds(pl.multiple_of(r * REST, REST), REST)] = s2
        return 0

    lax.fori_loop(0, 4, block, 0)
    spread(at, wa, tables[0], wo, slice(2 * CH, 3 * CH), slice(0, CH))
    spread(at, wb, tables[1], wo, slice(2 * CH, 3 * CH), slice(CH, 2 * CH))


def conv_edge_kernel(at, glu_a, glu_b, other, before, par_a, par_b, t1, t2, mixed, stats, win, l1, l2, *, layer):
    par_a, par_b = par_a.at[layer], par_b.at[layer]
    x, c = at[2], at[3]

    def block(r, _):
        idx = jnp.where(c == 1, r, (r + 1) % 4)
        first = jnp.logical_and(c == 0, r == x)
        here = pl.multiple_of(r * ROWS, KEEP)
        edge_at = pl.multiple_of(idx * KEEP, KEEP)
        s1 = jnp.zeros((KEEP, 128), F32)
        s2 = jnp.zeros((KEEP, 128), F32)
        for strip in range(4):
            lanes = slice((strip % 2) * 128, (strip % 2) * 128 + 128)
            there = slice(((strip + 2) % 4) * 128, ((strip + 2) % 4) * 128 + 128)
            glu, par = (glu_a, par_a) if strip < 2 else (glu_b, par_b)
            edge = other[pl.ds(edge_at, KEEP), there].astype(F32)
            win[0:KEEP] = jnp.where(first, before[:, there].astype(F32), edge)
            win[KEEP:] = glu[pl.ds(here, KEEP), lanes].astype(F32)
            acc = conv_strip(win, par, lanes, KEEP)
            mixed[pl.ds(pl.multiple_of(r * KEEP, KEEP), KEEP), strip * 128 : strip * 128 + 128] = acc
            s1 = s1 + acc
            s2 = s2 + acc * acc
        l1[pl.ds(pl.multiple_of(r * KEEP, KEEP), KEEP)] = s1
        l2[pl.ds(pl.multiple_of(r * KEEP, KEEP), KEEP)] = s2
        return 0

    lax.fori_loop(0, 4, block, 0)
    for o, low, high in ((0, l1, t1), (4, l2, t2)):
        for r in range(4):
            rows = [low[r * KEEP : (r + 1) * KEEP], high[r * REST : (r + 1) * REST]]
            rows = jnp.concatenate(rows + [jnp.zeros((128 - ROWS, 128), F32)], axis=0)
            stats[o + r : o + r + 1] = jnp.sum(rows.T, axis=0, keepdims=True)


def out_kernel(*refs, blocks, layer):
    at, low, high, stats, par_a, par_b, wo = refs[:7]
    outs, act = refs[7:-1], refs[-1]
    par_a, par_b = par_a.at[layer], par_b.at[layer]
    x = at[2]
    own, m, f, p = (stats[pl.ds(pl.multiple_of(((x + d) % 4) * 8, 8), 8)] for d in (0, 3, 2, 1))
    rows = []
    for o in (0, 4):
        for r in range(4):
            i, j, k = o + (r - 1) % 4, o + (r + 2) % 4, o + (r + 1) % 4
            rows.append(own[o + r : o + r + 1] + m[i : i + 1] + f[j : j + 1] + p[k : k + 1])
    mean = jnp.concatenate(rows[:4], axis=0) * (1.0 / CHANNELS)
    msq = jnp.concatenate(rows[4:], axis=0) * (1.0 / CHANNELS)
    inv = lax.rsqrt(msq - mean * mean + EPS)
    cols = jnp.concatenate([mean, inv], axis=0).T
    for n, r in enumerate(blocks):
        for src, size, first in ((low, KEEP, 0), (high, REST, KEEP)):
            mu = cols[first : first + size, r : r + 1]
            iv = cols[first : first + size, 4 + r : 5 + r]
            for s, par in ((0, par_a), (1, par_b)):
                v = (src[r * size : (r + 1) * size, s * CH : (s + 1) * CH] - mu) * iv
                v = v * par[TAPS + 1 : TAPS + 2] + par[TAPS + 2 : TAPS + 3]
                to = n * ROWS + first
                act[to : to + size, s * CH : (s + 1) * CH] = (v / (1.0 + jnp.exp(-v))).astype(BF)
    d = lax.dot_general(act[...], wo[...], (((1,), (1,)), ((), ())), preferred_element_type=F32)
    for n, out in enumerate(outs):
        out[...] = d[n * ROWS : (n + 1) * ROWS].astype(out.dtype)


def add_kernel(at, h, o0, m, p, f, out, *, last):
    for k in range(8):
        src = slice(k * CH, (k + 1) * CH)
        t = o0[:, src] + m[:, src].astype(F32) + p[:, src].astype(F32) + f[:, src].astype(F32)
        t = (h[:, src].astype(F32) + t).astype(BF)
        if last:
            out[:, pl.ds(pl.multiple_of(((at[0] + k) % 8) * CH, CH), CH)] = t
        else:
            out[:, src] = t


def out_call(layer, blocks, kinds, *inputs):
    return call(
        functools.partial(out_kernel, blocks=blocks, layer=layer),
        [((ROWS, WIDTH), k) for k in kinds],
        list(inputs),
        [pltpu.VMEM((len(blocks) * ROWS, 2 * CH), BF)],
    )


def layer_body(layer, at, state, tokens, own, other, par, before_pairs):
    glu_a, glu_b, tails, last = glu_calls(at, tokens, own, other)
    there = swap(tails)
    before = lax.ppermute(last, ("z", "y", "c"), before_pairs)
    par_a, par_b = par
    (a, ta), (b, tb) = own, other
    high, t1, t2, wo = call(
        functools.partial(conv_rest_kernel, n=len(a), m=len(b), tables=(ta, tb), layer=layer),
        [((4 * REST, 2 * CH), F32)] + [((4 * REST, 128), F32)] * 2 + [((WIDTH, 2 * CH), BF)],
        [at, glu_a, glu_b, par_a, par_b, *a, *b],
        [pltpu.VMEM((ROWS, 128), F32)],
    )
    low, s = call(
        functools.partial(conv_edge_kernel, layer=layer),
        [((4 * KEEP, 2 * CH), F32), ((8, 128), F32)],
        [at, glu_a, glu_b, there, before, par_a, par_b, t1, t2],
        [pltpu.VMEM((2 * KEEP, 128), F32)] + [pltpu.VMEM((4 * KEEP, 128), F32)] * 2,
    )
    stats = lax.all_to_all(jnp.broadcast_to(s[None], (4, 8, 128)), "x", 0, 0, tiled=True)
    inputs = (at, low, high, stats.reshape(32, 128), par_a, par_b, wo)
    (o2,) = out_call(layer, (2,), (BF,), *inputs)
    from_f = take(o2, "x", 2)
    o3, o1, o0 = out_call(layer, (3, 1, 0), (BF, BF, F32), *inputs)
    from_m, from_p = take(o3, "x", -1), take(o1, "x", 1)
    (state,) = call(
        functools.partial(add_kernel, last=layer == 1),
        [((ROWS, WIDTH), BF)],
        [at, state, o0, from_m, from_p, from_f],
    )
    return state, o1


def gather_tokens(h):
    m, p, f = take(h, "x", -1), take(h, "x", 1), take(h, "x", 2)
    return h, m, f, p


def body(hidden, norm_gain, w_value, w_gate, conv_weight, conv_bias, chan_gain, chan_shift, w_out):
    z, y, x, c = (lax.axis_index(a) for a in SP_TP)
    at = jnp.stack([z, y, x, c]).astype(jnp.int32)
    b0, b1 = call(
        fold_kernel,
        [((PIECE, BUNDLE), BF)] * 2,
        [at, norm_gain, w_value, w_gate, w_out.swapaxes(1, 2)],
        [pltpu.VMEM((128, 128), F32)],
    )
    (state,) = call(roll_kernel, [((ROWS, WIDTH), BF)], [at, hidden])
    (small,) = call(
        par_kernel,
        [((2, 40, CH), F32)],
        [conv_weight.swapaxes(0, 1), conv_bias, chan_gain, chan_shift],
        scalars=False,
    )

    za, zb, z4 = take(b0, "z", 1), take(b0, "z", -1), take(b0, "z", 4)
    z2 = take(jnp.concatenate([b0, za], axis=0), "z", 2)
    z6 = take(jnp.concatenate([b0, zb], axis=0), "z", -2)
    size, cut = 8 * PIECE, 4 * PIECE
    (line,) = call(line_kernel, [((size, BUNDLE), BF)], [b0, za, zb, z2, z4, z6], scalars=False)
    up, down = take(line, "y", 1), take(line, "y", -1)
    fu, fd = take(up[:cut], "y", 1), take(down[cut:], "y", -1)
    s2 = swap(jnp.concatenate([line, up, down], axis=0))
    s3 = swap(jnp.concatenate([fu, fd], axis=0))
    own0 = (
        [line, up, down, fu, fd],
        [(0, 0, (0, 0), size), (1, 0, (1, 0), size), (2, 0, (3, 0), size)]
        + [(3, 0, (2, 0), cut), (4, 0, (2, 4), cut)],
    )
    other0 = (
        [s2, s3],
        [(0, n * size, (dy, 0), size) for n, dy in enumerate((0, 1, 3))]
        + [(1, 0, (2, 0), size)],
    )

    g = [b1, take(b1, "y", 1), take(b1, "y", 2), take(b1, "y", 3)]
    (near,) = call(near_kernel, [((CH, BUNDLE), BF)], [at, *g])
    p1, m1 = take(near, "z", 1), take(near, "z", -1)
    p2, m2 = take(p1, "z", 1), take(m1, "z", -1)
    p3, m3 = take(p2, "z", 1), take(m2, "z", -1)
    p4 = take(p3, "z", 1)
    chunks = [near, p1, p2, p3, p4, m3, m2, m1]

    par = (small, swap(small))
    size = lax.axis_size("z") * lax.axis_size("y")
    pairs = [(2 * i + 1, 2 * (i + 1)) for i in range(size - 1)]
    state, ready = layer_body(0, at, state, gather_tokens(state), own0, other0, par, pairs)
    (both,) = call(cat_kernel, [((WIDTH, BUNDLE), BF)], [*chunks, ready], scalars=False)
    ysw = swap(both)
    own1 = (chunks, [(k, 0, k * CH, CH) for k in range(8)])
    other1 = ([ysw], [(0, 0, 0, WIDTH)])
    state, _ = layer_body(1, at, state, gather_tokens(state), own1, other1, par, pairs)
    return state


def solution(mesh):
    torus = Mesh(mesh.devices.reshape(8, 4, 4, 2), SP_TP)
    tp = ("x", "c")
    in_specs = (
        P(SP_TP, None),
        P(),
        P(None, SP, tp),
        P(None, SP, tp),
        P(None, None, tp),
        P(None, tp),
        P(None, tp),
        P(None, tp),
        P(None, tp, SP),
    )
    return jax.shard_map(
        body, mesh=torus, in_specs=in_specs, out_specs=P(SP_TP, None), check_vma=False
    )
```

```python
import functools

import jax
import jax.numpy as jnp
from jax import lax
from jax.experimental import pallas as pl
from jax.experimental.pallas import tpu as pltpu
from jax.sharding import Mesh
from jax.sharding import PartitionSpec as P


SP = ("z", "y")
SP_TP = ("z", "y", "x", "c")
EPS = 1e-06
BF = jnp.bfloat16
F32 = jnp.float32
ROWS = 96
CH = 256
TAPS = 31
KEEP = 32
REST = ROWS - KEEP
WIDTH = 2048
CHANNELS = 2048
BUNDLE = 3 * CH
PIECE = 64


def take(a, axis, by):
    n = lax.axis_size(axis)
    return lax.ppermute(a, axis, [((i + by) % n, i) for i in range(n)])


def swap(a):
    return lax.ppermute(a, "c", [(0, 1), (1, 0)])


def call(kernel, outs, inputs, scratch=(), scalars=True, alias=None):
    n = len(inputs) - (1 if scalars else 0)
    vmem = pl.BlockSpec(memory_space=pltpu.VMEM)
    specs = ([pl.BlockSpec(memory_space=pltpu.SMEM)] if scalars else []) + [vmem] * n
    return pl.pallas_call(
        kernel,
        out_shape=[jax.ShapeDtypeStruct(s, d) for s, d in outs],
        in_specs=specs,
        out_specs=[vmem] * len(outs),
        scratch_shapes=list(scratch),
        input_output_aliases=alias or {},
        compiler_params=pltpu.CompilerParams(vmem_limit_bytes=12 * 1024 * 1024),
    )(*inputs)


def fold_kernel(at, gain, wv, wg, wo, b0, b1, col):
    sp = at[0] * 4 + at[1]
    for layer, out in ((0, b0), (1, b1)):
        lane = pl.multiple_of((sp // 2) * 128, 128)
        g = gain[layer : layer + 1, pl.ds(lane, 128)]
        col[...] = jnp.broadcast_to(g, (128, 128)).T
        g = col[pl.ds(pl.multiple_of((sp % 2) * PIECE, PIECE), PIECE), 0:1]
        out[:, :CH] = (wv[layer].astype(F32) * g).astype(BF)
        out[:, CH : 2 * CH] = (wg[layer].astype(F32) * g).astype(BF)
        out[:, 2 * CH :] = wo[layer]


def roll_kernel(at, hidden, state):
    for k in range(8):
        src = pl.multiple_of(((at[0] + k) % 8) * CH, CH)
        state[:, k * CH : (k + 1) * CH] = hidden[:, pl.ds(src, CH)]


def par_kernel(cw, cb, cg, cs, par):
    for layer in range(2):
        par[layer, :TAPS] = cw[:, layer]
        for n, a in enumerate((cb, cg, cs)):
            par[layer, TAPS + n : TAPS + n + 1] = a[layer : layer + 1]


def near_kernel(at, a0, a1, a2, a3, out):
    y = at[1]
    for k, a in enumerate((a0, a1, a2, a3)):
        out[pl.ds(pl.multiple_of(((y + k) % 4) * PIECE, PIECE), PIECE)] = a[...]


def line_kernel(own, za, zb, z2, z4, z6, out):
    pieces = (own, za, z2.at[:PIECE], z2.at[PIECE:], z4, z6.at[PIECE:], z6.at[:PIECE], zb)
    for k, a in enumerate(pieces):
        out[k * PIECE : (k + 1) * PIECE] = a[...]


def cat_kernel(*refs):
    out = refs[-1]
    for k, a in enumerate(refs[:8]):
        out[k * CH : (k + 1) * CH] = a[...]


def spread_kernel(at, *refs, table):
    out = refs[-1]
    for i, row, dy, first, n in table:
        base = first * CH + ((at[1] + dy) % 4) * PIECE

        def piece(j, _, i=i, row=row, base=base):
            src = pl.multiple_of(row + j * PIECE, PIECE)
            to = pl.multiple_of(base + j * CH, PIECE)
            out[pl.ds(to, PIECE)] = refs[i][pl.ds(src, PIECE)]
            return 0

        lax.fori_loop(0, n, piece, 0)


def spread_call(at, arrays, table, into=None):
    inputs = [at, *arrays] + ([] if into is None else [into])
    return call(
        functools.partial(spread_kernel, table=table),
        [((WIDTH, BUNDLE), BF)],
        inputs,
        alias=None if into is None else {len(inputs) - 1: 0},
    )[0]


def tok_kernel(own, m, f, p, tok, scale):
    for r, a in enumerate((own, m, f, p)):
        tok[r * ROWS : (r + 1) * ROWS] = a[...]
        t = jnp.zeros((ROWS, 128), F32)
        for k in range(WIDTH // 128):
            v = a[:, k * 128 : (k + 1) * 128].astype(F32)
            t = t + v * v
        s = lax.rsqrt(jnp.sum(t, axis=1, keepdims=True) * (1.0 / WIDTH) + EPS)
        scale[r * ROWS : (r + 1) * ROWS] = jnp.broadcast_to(s, (ROWS, 128))


def glu_of(tok, scale, w):
    both = jnp.dot(tok[...], w[:, : 2 * CH], preferred_element_type=F32)
    s = scale[:, 0:1]
    lin, gate = both[:, :CH] * s, both[:, CH:] * s
    return (lin / (1.0 + jnp.exp(-gate))).astype(BF)


def glu_first_kernel(tok, scale, w, glu):
    glu[...] = glu_of(tok, scale, w)


def glu_second_kernel(at, tok, scale, other, w, glu, tails, last):
    glu[...] = glu_of(tok, scale, w)
    for r in range(4):
        here = slice((r + 1) * ROWS - KEEP, (r + 1) * ROWS)
        tails[r * KEEP : (r + 1) * KEEP, :CH] = other[here]
        tails[r * KEEP : (r + 1) * KEEP, CH:] = glu[here]
    last[...] = tails[pl.ds(pl.multiple_of(((at[2] + 1) % 4) * KEEP, KEEP), KEEP)]


def glu_calls(at, tokens, own, other):
    size = (4 * ROWS, CH)
    tok, scale = call(
        tok_kernel, [((4 * ROWS, WIDTH), BF), ((4 * ROWS, 128), F32)], list(tokens), scalars=False
    )
    (glu_a,) = call(glu_first_kernel, [(size, BF)], [tok, scale, own], scalars=False)
    glu_b, tails, last = call(
        glu_second_kernel,
        [(size, BF), ((4 * KEEP, 2 * CH), BF), ((KEEP, 2 * CH), BF)],
        [at, tok, scale, glu_a, other],
    )
    return glu_a, glu_b, tails, last


def conv_strip(win, par, lanes, rows):
    acc = jnp.zeros((rows, 128), F32) + par[TAPS : TAPS + 1, lanes]
    for s in range(8):
        shifted = win[s : s + rows + (24 if s else 32)]
        for base in range(0, 40, 8):
            tap = base + s - (KEEP - (TAPS - 1))
            if 0 <= tap < TAPS:
                acc = acc + par[tap : tap + 1, lanes] * shifted[base : base + rows]
    return acc


def conv_rest_kernel(glu_a, glu_b, par_a, par_b, mixed, t1, t2, win, *, layer):
    par_a, par_b = par_a.at[layer], par_b.at[layer]

    def block(r, _):
        here = pl.multiple_of(r * ROWS, KEEP)
        s1 = jnp.zeros((REST, 128), F32)
        s2 = jnp.zeros((REST, 128), F32)
        for strip in range(4):
            lanes = slice((strip % 2) * 128, (strip % 2) * 128 + 128)
            glu, par = (glu_a, par_a) if strip < 2 else (glu_b, par_b)
            win[...] = glu[pl.ds(here, ROWS), lanes].astype(F32)
            acc = conv_strip(win, par, lanes, REST)
            mixed[pl.ds(pl.multiple_of(r * REST, REST), REST), strip * 128 : strip * 128 + 128] = acc
            s1 = s1 + acc
            s2 = s2 + acc * acc
        t1[pl.ds(pl.multiple_of(r * REST, REST), REST)] = s1
        t2[pl.ds(pl.multiple_of(r * REST, REST), REST)] = s2
        return 0

    lax.fori_loop(0, 4, block, 0)


def conv_edge_kernel(at, glu_a, glu_b, other, before, par_a, par_b, t1, t2, mixed, stats, win, l1, l2, *, layer):
    par_a, par_b = par_a.at[layer], par_b.at[layer]
    x, c = at[2], at[3]

    def block(r, _):
        idx = jnp.where(c == 1, r, (r + 1) % 4)
        first = jnp.logical_and(c == 0, r == x)
        here = pl.multiple_of(r * ROWS, KEEP)
        edge_at = pl.multiple_of(idx * KEEP, KEEP)
        s1 = jnp.zeros((KEEP, 128), F32)
        s2 = jnp.zeros((KEEP, 128), F32)
        for strip in range(4):
            lanes = slice((strip % 2) * 128, (strip % 2) * 128 + 128)
            there = slice(((strip + 2) % 4) * 128, ((strip + 2) % 4) * 128 + 128)
            glu, par = (glu_a, par_a) if strip < 2 else (glu_b, par_b)
            edge = other[pl.ds(edge_at, KEEP), there].astype(F32)
            win[0:KEEP] = jnp.where(first, before[:, there].astype(F32), edge)
            win[KEEP:] = glu[pl.ds(here, KEEP), lanes].astype(F32)
            acc = conv_strip(win, par, lanes, KEEP)
            mixed[pl.ds(pl.multiple_of(r * KEEP, KEEP), KEEP), strip * 128 : strip * 128 + 128] = acc
            s1 = s1 + acc
            s2 = s2 + acc * acc
        l1[pl.ds(pl.multiple_of(r * KEEP, KEEP), KEEP)] = s1
        l2[pl.ds(pl.multiple_of(r * KEEP, KEEP), KEEP)] = s2
        return 0

    lax.fori_loop(0, 4, block, 0)
    for o, low, high in ((0, l1, t1), (4, l2, t2)):
        for r in range(4):
            rows = [low[r * KEEP : (r + 1) * KEEP], high[r * REST : (r + 1) * REST]]
            rows = jnp.concatenate(rows + [jnp.zeros((128 - ROWS, 128), F32)], axis=0)
            stats[o + r : o + r + 1] = jnp.sum(rows.T, axis=0, keepdims=True)


def out_kernel(*refs, blocks, layer):
    at, low, high, stats, par_a, par_b, wa, wb = refs[:8]
    outs, act = refs[8:-1], refs[-1]
    par_a, par_b = par_a.at[layer], par_b.at[layer]
    x = at[2]
    own, m, f, p = (stats[pl.ds(pl.multiple_of(((x + d) % 4) * 8, 8), 8)] for d in (0, 3, 2, 1))
    rows = []
    for o in (0, 4):
        for r in range(4):
            i, j, k = o + (r - 1) % 4, o + (r + 2) % 4, o + (r + 1) % 4
            rows.append(own[o + r : o + r + 1] + m[i : i + 1] + f[j : j + 1] + p[k : k + 1])
    mean = jnp.concatenate(rows[:4], axis=0) * (1.0 / CHANNELS)
    msq = jnp.concatenate(rows[4:], axis=0) * (1.0 / CHANNELS)
    inv = lax.rsqrt(msq - mean * mean + EPS)
    cols = jnp.concatenate([mean, inv], axis=0).T
    for n, r in enumerate(blocks):
        for src, size, first in ((low, KEEP, 0), (high, REST, KEEP)):
            mu = cols[first : first + size, r : r + 1]
            iv = cols[first : first + size, 4 + r : 5 + r]
            for s, par in ((0, par_a), (1, par_b)):
                v = (src[r * size : (r + 1) * size, s * CH : (s + 1) * CH] - mu) * iv
                v = v * par[TAPS + 1 : TAPS + 2] + par[TAPS + 2 : TAPS + 3]
                to = n * ROWS + first
                act[to : to + size, s * CH : (s + 1) * CH] = (v / (1.0 + jnp.exp(-v))).astype(BF)
    dims = (((1,), (1,)), ((), ()))
    d = lax.dot_general(act[:, :CH], wa[:, 2 * CH :], dims, preferred_element_type=F32)
    d = d + lax.dot_general(act[:, CH:], wb[:, 2 * CH :], dims, preferred_element_type=F32)
    for n, out in enumerate(outs):
        out[...] = d[n * ROWS : (n + 1) * ROWS].astype(out.dtype)


def add_kernel(at, h, o0, m, p, f, out, *, last):
    for k in range(8):
        src = slice(k * CH, (k + 1) * CH)
        t = o0[:, src] + m[:, src].astype(F32) + p[:, src].astype(F32) + f[:, src].astype(F32)
        t = (h[:, src].astype(F32) + t).astype(BF)
        if last:
            out[:, pl.ds(pl.multiple_of(((at[0] + k) % 8) * CH, CH), CH)] = t
        else:
            out[:, src] = t


def out_call(layer, blocks, kinds, *inputs):
    return call(
        functools.partial(out_kernel, blocks=blocks, layer=layer),
        [((ROWS, WIDTH), k) for k in kinds],
        list(inputs),
        [pltpu.VMEM((len(blocks) * ROWS, 2 * CH), BF)],
    )


def layer_body(layer, at, state, tokens, own, other, par, before_pairs):
    glu_a, glu_b, tails, last = glu_calls(at, tokens, own, other)
    there = swap(tails)
    before = lax.ppermute(last, ("z", "y", "c"), before_pairs)
    par_a, par_b = par
    high, t1, t2 = call(
        functools.partial(conv_rest_kernel, layer=layer),
        [((4 * REST, 2 * CH), F32)] + [((4 * REST, 128), F32)] * 2,
        [glu_a, glu_b, par_a, par_b],
        [pltpu.VMEM((ROWS, 128), F32)],
        scalars=False,
    )
    low, s = call(
        functools.partial(conv_edge_kernel, layer=layer),
        [((4 * KEEP, 2 * CH), F32), ((8, 128), F32)],
        [at, glu_a, glu_b, there, before, par_a, par_b, t1, t2],
        [pltpu.VMEM((2 * KEEP, 128), F32)] + [pltpu.VMEM((4 * KEEP, 128), F32)] * 2,
    )
    stats = lax.all_to_all(jnp.broadcast_to(s[None], (4, 8, 128)), "x", 0, 0, tiled=True)
    inputs = (at, low, high, stats.reshape(32, 128), par_a, par_b, own, other)
    (o2,) = out_call(layer, (2,), (BF,), *inputs)
    from_f = take(o2, "x", 2)
    o3, o1, o0 = out_call(layer, (3, 1, 0), (BF, BF, F32), *inputs)
    from_m, from_p = take(o3, "x", -1), take(o1, "x", 1)
    (state,) = call(
        functools.partial(add_kernel, last=layer == 1),
        [((ROWS, WIDTH), BF)],
        [at, state, o0, from_m, from_p, from_f],
    )
    return state, o1


def gather_tokens(h):
    m, p, f = take(h, "x", -1), take(h, "x", 1), take(h, "x", 2)
    return h, m, f, p


def body(hidden, norm_gain, w_value, w_gate, conv_weight, conv_bias, chan_gain, chan_shift, w_out):
    z, y, x, c = (lax.axis_index(a) for a in SP_TP)
    at = jnp.stack([z, y, x, c]).astype(jnp.int32)
    b0, b1 = call(
        fold_kernel,
        [((PIECE, BUNDLE), BF)] * 2,
        [at, norm_gain, w_value, w_gate, w_out.swapaxes(1, 2)],
        [pltpu.VMEM((128, 128), F32)],
    )
    (state,) = call(roll_kernel, [((ROWS, WIDTH), BF)], [at, hidden])
    (small,) = call(
        par_kernel,
        [((2, 40, CH), F32)],
        [conv_weight.swapaxes(0, 1), conv_bias, chan_gain, chan_shift],
        scalars=False,
    )

    za, zb, z4 = take(b0, "z", 1), take(b0, "z", -1), take(b0, "z", 4)
    z2 = take(jnp.concatenate([b0, za], axis=0), "z", 2)
    z6 = take(jnp.concatenate([b0, zb], axis=0), "z", -2)
    size, cut = 8 * PIECE, 4 * PIECE
    (line,) = call(line_kernel, [((size, BUNDLE), BF)], [b0, za, zb, z2, z4, z6], scalars=False)
    up, down = take(line, "y", 1), take(line, "y", -1)
    fu, fd = take(up[:cut], "y", 1), take(down[cut:], "y", -1)
    s2 = swap(jnp.concatenate([line, up, down], axis=0))
    s3 = swap(jnp.concatenate([fu, fd], axis=0))
    own0 = spread_call(at, [line, up, down], ((0, 0, 0, 0, 8), (1, 0, 1, 0, 8), (2, 0, 3, 0, 8)))
    own0 = spread_call(at, [fu, fd], ((0, 0, 2, 0, 4), (1, 0, 2, 4, 4)), own0)
    table = ((0, 0, 0, 0, 8), (0, size, 1, 0, 8), (0, 2 * size, 3, 0, 8), (1, 0, 2, 0, 8))
    other0 = spread_call(at, [s2, s3], table)

    g = [b1, take(b1, "y", 1), take(b1, "y", 2), take(b1, "y", 3)]
    (near,) = call(near_kernel, [((CH, BUNDLE), BF)], [at, *g])
    p1, m1 = take(near, "z", 1), take(near, "z", -1)
    p2, m2 = take(p1, "z", 1), take(m1, "z", -1)
    p3, m3 = take(p2, "z", 1), take(m2, "z", -1)
    p4 = take(p3, "z", 1)
    chunks = [near, p1, p2, p3, p4, m3, m2, m1]

    par = (small, swap(small))
    size = lax.axis_size("z") * lax.axis_size("y")
    pairs = [(2 * i + 1, 2 * (i + 1)) for i in range(size - 1)]
    state, ready = layer_body(0, at, state, gather_tokens(state), own0, other0, par, pairs)
    (own1,) = call(cat_kernel, [((WIDTH, BUNDLE), BF)], [*chunks, ready], scalars=False)
    other1 = swap(own1)
    state, _ = layer_body(1, at, state, gather_tokens(state), own1, other1, par, pairs)
    return state


def solution(mesh):
    torus = Mesh(mesh.devices.reshape(8, 4, 4, 2), SP_TP)
    tp = ("x", "c")
    in_specs = (
        P(SP_TP, None),
        P(),
        P(None, SP, tp),
        P(None, SP, tp),
        P(None, None, tp),
        P(None, tp),
        P(None, tp),
        P(None, tp),
        P(None, tp, SP),
    )
    return jax.shard_map(
        body, mesh=torus, in_specs=in_specs, out_specs=P(SP_TP, None), check_vma=False
    )
```

```python
import functools

import jax
import jax.numpy as jnp
from jax import lax
from jax.experimental import pallas as pl
from jax.experimental.pallas import tpu as pltpu
from jax.sharding import Mesh
from jax.sharding import PartitionSpec as P


SP = ("z", "y")
SP_TP = ("z", "y", "x", "c")
EPS = 1e-06
BF = jnp.bfloat16
F32 = jnp.float32
ROWS = 96
CH = 256
TAPS = 31
KEEP = 32
REST = ROWS - KEEP
WIDTH = 2048
CHANNELS = 2048
BUNDLE = 3 * CH
PIECE = 64


HALF = WIDTH // 2


def take(a, axis, by):
    n = lax.axis_size(axis)
    return lax.ppermute(a, axis, [((i + by) % n, i) for i in range(n)])


def swap(a):
    return lax.ppermute(a, "c", [(0, 1), (1, 0)])


def call(kernel, outs, inputs, scratch=(), scalars=True, alias=None):
    n = len(inputs) - (1 if scalars else 0)
    vmem = pl.BlockSpec(memory_space=pltpu.VMEM)
    specs = ([pl.BlockSpec(memory_space=pltpu.SMEM)] if scalars else []) + [vmem] * n
    return pl.pallas_call(
        kernel,
        out_shape=[jax.ShapeDtypeStruct(s, d) for s, d in outs],
        in_specs=specs,
        out_specs=[vmem] * len(outs),
        scratch_shapes=list(scratch),
        input_output_aliases=alias or {},
        compiler_params=pltpu.CompilerParams(vmem_limit_bytes=12 * 1024 * 1024),
    )(*inputs)


def fold_kernel(at, gain, wv, wg, wo, b0, b1, col):
    sp = at[0] * 4 + at[1]
    for layer, out in ((0, b0), (1, b1)):
        lane = pl.multiple_of((sp // 2) * 128, 128)
        g = gain[layer : layer + 1, pl.ds(lane, 128)]
        col[...] = jnp.broadcast_to(g, (128, 128)).T
        g = col[pl.ds(pl.multiple_of((sp % 2) * PIECE, PIECE), PIECE), 0:1]
        out[:, :CH] = (wv[layer].astype(F32) * g).astype(BF)
        out[:, CH : 2 * CH] = (wg[layer].astype(F32) * g).astype(BF)
        out[:, 2 * CH :] = wo[layer]


def roll_kernel(at, hidden, state):
    for k in range(8):
        src = pl.multiple_of(((at[0] + k) % 8) * CH, CH)
        state[:, k * CH : (k + 1) * CH] = hidden[:, pl.ds(src, CH)]


def par_kernel(cw, cb, cg, cs, par):
    for layer in range(2):
        par[layer, :TAPS] = cw[:, layer]
        for n, a in enumerate((cb, cg, cs)):
            par[layer, TAPS + n : TAPS + n + 1] = a[layer : layer + 1]


def near_kernel(at, a0, a1, a2, a3, out):
    y = at[1]
    for k, a in enumerate((a0, a1, a2, a3)):
        out[pl.ds(pl.multiple_of(((y + k) % 4) * PIECE, PIECE), PIECE)] = a[...]


def line_kernel(own, za, zb, z2, z4, z6, out, wo):
    pieces = (own, za, z2.at[:PIECE], z2.at[PIECE:], z4, z6.at[PIECE:], z6.at[:PIECE], zb)
    for k, a in enumerate(pieces):
        out[k * PIECE : (k + 1) * PIECE] = a[:, : 2 * CH]
        wo[k * PIECE : (k + 1) * PIECE] = a[:, 2 * CH :]


def cat_kernel(*refs, n):
    out, at = refs[-1], 0
    for a in refs[:n]:
        out[at : at + a.shape[0]] = a[...]
        at += a.shape[0]


def spread_kernel(at, *refs, table):
    out = refs[-1]
    for i, row, dy, first, n in table:
        base = first * CH + ((at[1] + dy) % 4) * PIECE

        def piece(j, _, i=i, row=row, base=base):
            src = pl.multiple_of(row + j * PIECE, PIECE)
            to = pl.multiple_of(base + j * CH, PIECE)
            out[pl.ds(to, PIECE)] = refs[i][pl.ds(src, PIECE)]
            return 0

        lax.fori_loop(0, n, piece, 0)


def spread_call(at, arrays, table, into=None):
    inputs = [at, *arrays] + ([] if into is None else [into])
    return call(
        functools.partial(spread_kernel, table=table),
        [((WIDTH, arrays[0].shape[1]), BF)],
        inputs,
        alias=None if into is None else {len(inputs) - 1: 0},
    )[0]


def tok_kernel(*refs, counts):
    tok, scale = refs[-2:]
    at = 0
    for r, n in enumerate(counts):
        t = jnp.zeros((ROWS, 128), F32)
        cols = WIDTH // n
        for i, a in enumerate(refs[at : at + n]):
            tok[r * ROWS : (r + 1) * ROWS, i * cols : (i + 1) * cols] = a[...]
            for k in range(cols // 128):
                v = a[:, k * 128 : (k + 1) * 128].astype(F32)
                t = t + v * v
        at += n
        s = lax.rsqrt(jnp.sum(t, axis=1, keepdims=True) * (1.0 / WIDTH) + EPS)
        scale[r * ROWS : (r + 1) * ROWS] = jnp.broadcast_to(s, (ROWS, 128))


def glu_of(tok, scale, w):
    both = jnp.dot(tok[...], w[:, : 2 * CH], preferred_element_type=F32)
    s = scale[:, 0:1]
    lin, gate = both[:, :CH] * s, both[:, CH:] * s
    return (lin / (1.0 + jnp.exp(-gate))).astype(BF)


def glu_first_kernel(tok, scale, w, glu):
    glu[...] = glu_of(tok, scale, w)


def glu_second_kernel(at, tok, scale, other, w, glu, tails, last):
    glu[...] = glu_of(tok, scale, w)
    for r in range(4):
        here = slice((r + 1) * ROWS - KEEP, (r + 1) * ROWS)
        tails[r * KEEP : (r + 1) * KEEP, :CH] = other[here]
        tails[r * KEEP : (r + 1) * KEEP, CH:] = glu[here]
    last[...] = tails[pl.ds(pl.multiple_of(((at[2] + 1) % 4) * KEEP, KEEP), KEEP)]


def glu_calls(at, tokens, own, other):
    size = (4 * ROWS, CH)
    tok, scale = call(
        functools.partial(tok_kernel, counts=tuple(len(t) for t in tokens)),
        [((4 * ROWS, WIDTH), BF), ((4 * ROWS, 128), F32)],
        [a for t in tokens for a in t],
        scalars=False,
    )
    (glu_a,) = call(glu_first_kernel, [(size, BF)], [tok, scale, own], scalars=False)
    glu_b, tails, last = call(
        glu_second_kernel,
        [(size, BF), ((4 * KEEP, 2 * CH), BF), ((KEEP, 2 * CH), BF)],
        [at, tok, scale, glu_a, other],
    )
    return glu_a, glu_b, tails, last


def conv_strip(win, par, lanes, rows):
    acc = jnp.zeros((rows, 128), F32) + par[TAPS : TAPS + 1, lanes]
    for s in range(8):
        shifted = win[s : s + rows + (24 if s else 32)]
        for base in range(0, 40, 8):
            tap = base + s - (KEEP - (TAPS - 1))
            if 0 <= tap < TAPS:
                acc = acc + par[tap : tap + 1, lanes] * shifted[base : base + rows]
    return acc


def conv_rest_kernel(glu_a, glu_b, par_a, par_b, mixed, t1, t2, win, *, layer):
    par_a, par_b = par_a.at[layer], par_b.at[layer]

    def block(r, _):
        here = pl.multiple_of(r * ROWS, KEEP)
        s1 = jnp.zeros((REST, 128), F32)
        s2 = jnp.zeros((REST, 128), F32)
        for strip in range(4):
            lanes = slice((strip % 2) * 128, (strip % 2) * 128 + 128)
            glu, par = (glu_a, par_a) if strip < 2 else (glu_b, par_b)
            win[...] = glu[pl.ds(here, ROWS), lanes].astype(F32)
            acc = conv_strip(win, par, lanes, REST)
            mixed[pl.ds(pl.multiple_of(r * REST, REST), REST), strip * 128 : strip * 128 + 128] = acc
            s1 = s1 + acc
            s2 = s2 + acc * acc
        t1[pl.ds(pl.multiple_of(r * REST, REST), REST)] = s1
        t2[pl.ds(pl.multiple_of(r * REST, REST), REST)] = s2
        return 0

    lax.fori_loop(0, 4, block, 0)


def conv_edge_kernel(at, glu_a, glu_b, other, before, par_a, par_b, t1, t2, mixed, stats, win, l1, l2, *, layer):
    par_a, par_b = par_a.at[layer], par_b.at[layer]
    x, c = at[2], at[3]

    def block(r, _):
        idx = jnp.where(c == 1, r, (r + 1) % 4)
        first = jnp.logical_and(c == 0, r == x)
        here = pl.multiple_of(r * ROWS, KEEP)
        edge_at = pl.multiple_of(idx * KEEP, KEEP)
        s1 = jnp.zeros((KEEP, 128), F32)
        s2 = jnp.zeros((KEEP, 128), F32)
        for strip in range(4):
            lanes = slice((strip % 2) * 128, (strip % 2) * 128 + 128)
            there = slice(((strip + 2) % 4) * 128, ((strip + 2) % 4) * 128 + 128)
            glu, par = (glu_a, par_a) if strip < 2 else (glu_b, par_b)
            edge = other[pl.ds(edge_at, KEEP), there].astype(F32)
            win[0:KEEP] = jnp.where(first, before[:, there].astype(F32), edge)
            win[KEEP:] = glu[pl.ds(here, KEEP), lanes].astype(F32)
            acc = conv_strip(win, par, lanes, KEEP)
            mixed[pl.ds(pl.multiple_of(r * KEEP, KEEP), KEEP), strip * 128 : strip * 128 + 128] = acc
            s1 = s1 + acc
            s2 = s2 + acc * acc
        l1[pl.ds(pl.multiple_of(r * KEEP, KEEP), KEEP)] = s1
        l2[pl.ds(pl.multiple_of(r * KEEP, KEEP), KEEP)] = s2
        return 0

    lax.fori_loop(0, 4, block, 0)
    for o, low, high in ((0, l1, t1), (4, l2, t2)):
        for r in range(4):
            rows = [low[r * KEEP : (r + 1) * KEEP], high[r * REST : (r + 1) * REST]]
            rows = jnp.concatenate(rows + [jnp.zeros((128 - ROWS, 128), F32)], axis=0)
            stats[o + r : o + r + 1] = jnp.sum(rows.T, axis=0, keepdims=True)


def out_kernel(*refs, blocks, places, layer):
    low, high, own, m, p, f, par_a, par_b, wa, wb = refs[:10]
    outs, act = refs[10:-1], refs[-1]
    par_a, par_b = par_a.at[layer], par_b.at[layer]
    rows = []
    for o in (0, 4):
        for r in range(4):
            i, j, k = o + (r - 1) % 4, o + (r + 2) % 4, o + (r + 1) % 4
            rows.append(own[o + r : o + r + 1] + m[i : i + 1] + f[j : j + 1] + p[k : k + 1])
    mean = jnp.concatenate(rows[:4], axis=0) * (1.0 / CHANNELS)
    msq = jnp.concatenate(rows[4:], axis=0) * (1.0 / CHANNELS)
    inv = lax.rsqrt(msq - mean * mean + EPS)
    cols = jnp.concatenate([mean, inv], axis=0).T
    for n, r in enumerate(blocks):
        for src, size, first in ((low, KEEP, 0), (high, REST, KEEP)):
            mu = cols[first : first + size, r : r + 1]
            iv = cols[first : first + size, 4 + r : 5 + r]
            for s, par in ((0, par_a), (1, par_b)):
                v = (src[r * size : (r + 1) * size, s * CH : (s + 1) * CH] - mu) * iv
                v = v * par[TAPS + 1 : TAPS + 2] + par[TAPS + 2 : TAPS + 3]
                to = n * ROWS + first
                act[to : to + size, s * CH : (s + 1) * CH] = (v / (1.0 + jnp.exp(-v))).astype(BF)
    dims = (((1,), (1,)), ((), ()))
    d = lax.dot_general(act[:, :CH], wa[:, wa.shape[1] - CH :], dims, preferred_element_type=F32)
    d = d + lax.dot_general(act[:, CH:], wb[:, wb.shape[1] - CH :], dims, preferred_element_type=F32)
    for out, (n, first) in zip(outs, places):
        out[...] = d[n * ROWS : (n + 1) * ROWS, first : first + out.shape[1]].astype(out.dtype)


def add_kernel(at, h, o0, ql, ml, pr, qr, *outs, last):
    for k in range(8):
        src = slice(k * CH, (k + 1) * CH)
        to = slice((k % 4) * CH, (k % 4 + 1) * CH)
        a, b = (ql, ml) if k < 4 else (pr, qr)
        t = o0[:, src] + a[:, to].astype(F32) + b[:, to].astype(F32)
        t = (h[:, src].astype(F32) + t).astype(BF)
        if last:
            outs[0][:, pl.ds(pl.multiple_of(((at[0] + k) % 8) * CH, CH), CH)] = t
        else:
            outs[0][:, src] = t
            outs[1 + k // 4][:, to] = t


def merge_kernel(a, b, out):
    out[...] = (a[...].astype(F32) + b[...].astype(F32)).astype(BF)


def out_call(layer, blocks, places, outs, *inputs):
    return call(
        functools.partial(out_kernel, blocks=blocks, places=places, layer=layer),
        outs,
        list(inputs),
        [pltpu.VMEM((len(blocks) * ROWS, 2 * CH), BF)],
        scalars=False,
    )


def layer_body(layer, at, state, tokens, own, other, wo_own, wo_other, par, before_pairs):
    glu_a, glu_b, tails, last = glu_calls(at, tokens, own, other)
    there = swap(tails)
    before = lax.ppermute(last, ("z", "y", "c"), before_pairs)
    par_a, par_b = par
    high, t1, t2 = call(
        functools.partial(conv_rest_kernel, layer=layer),
        [((4 * REST, 2 * CH), F32)] + [((4 * REST, 128), F32)] * 2,
        [glu_a, glu_b, par_a, par_b],
        [pltpu.VMEM((ROWS, 128), F32)],
        scalars=False,
    )
    low, s = call(
        functools.partial(conv_edge_kernel, layer=layer),
        [((4 * KEEP, 2 * CH), F32), ((8, 128), F32)],
        [at, glu_a, glu_b, there, before, par_a, par_b, t1, t2],
        [pltpu.VMEM((2 * KEEP, 128), F32)] + [pltpu.VMEM((4 * KEEP, 128), F32)] * 2,
    )
    stats = (s, take(s, "x", -1), take(s, "x", 1), take(s, "x", 2))
    if callable(wo_other):
        wo_other = wo_other()
    inputs = (low, high, *stats, par_a, par_b, wo_own, wo_other)
    piece = ((ROWS, HALF), BF)
    far_l, far_r = out_call(layer, (2,), ((0, 0), (0, HALF)), [piece] * 2, *inputs)
    far_l, far_r = take(far_l, "x", -1), take(far_r, "x", 1)
    o3l, o3r, o1l, o1r, o0 = out_call(
        layer,
        (3, 1, 0),
        ((0, 0), (0, HALF), (1, 0), (1, HALF), (2, 0)),
        [piece] * 4 + [((ROWS, WIDTH), F32)],
        *inputs,
    )
    pr, ml = take(o3r, "x", -1), take(o1l, "x", 1)
    (sum_l,) = call(merge_kernel, [piece], [o3l, far_l], scalars=False)
    (sum_r,) = call(merge_kernel, [piece], [o1r, far_r], scalars=False)
    ql, qr = take(sum_l, "x", -1), take(sum_r, "x", 1)
    outs = [((ROWS, WIDTH), BF)] + ([piece] * 2 if layer == 0 else [])
    state = call(
        functools.partial(add_kernel, last=layer == 1), outs, [at, state, o0, ql, ml, pr, qr]
    )
    return state, o3l


def gather_tokens(h):
    m, p, f = take(h, "x", -1), take(h, "x", 1), take(h, "x", 2)
    return (h,), (m,), (f,), (p,)


def gather_halves(h, left, right):
    ml, pr = take(left, "x", -1), take(right, "x", 1)
    mr, pl_ = take(right, "x", -1), take(left, "x", 1)
    fl, fr = take(ml, "x", -1), take(pr, "x", 1)
    return (h,), (ml, mr), (fl, fr), (pl_, pr)


def body(hidden, norm_gain, w_value, w_gate, conv_weight, conv_bias, chan_gain, chan_shift, w_out):
    z, y, x, c = (lax.axis_index(a) for a in SP_TP)
    at = jnp.stack([z, y, x, c]).astype(jnp.int32)
    b0, b1 = call(
        fold_kernel,
        [((PIECE, BUNDLE), BF)] * 2,
        [at, norm_gain, w_value, w_gate, w_out.swapaxes(1, 2)],
        [pltpu.VMEM((128, 128), F32)],
    )
    (state,) = call(roll_kernel, [((ROWS, WIDTH), BF)], [at, hidden])
    (small,) = call(
        par_kernel,
        [((2, 40, CH), F32)],
        [conv_weight.swapaxes(0, 1), conv_bias, chan_gain, chan_shift],
        scalars=False,
    )

    za, zb, z4 = take(b0, "z", 1), take(b0, "z", -1), take(b0, "z", 4)
    z2 = take(jnp.concatenate([b0, za], axis=0), "z", 2)
    z6 = take(jnp.concatenate([b0, zb], axis=0), "z", -2)
    size, cut = 8 * PIECE, 4 * PIECE
    line, wline = call(
        line_kernel,
        [((size, 2 * CH), BF), ((size, CH), BF)],
        [b0, za, zb, z2, z4, z6],
        scalars=False,
    )
    up, down = take(line, "y", 1), take(line, "y", -1)
    fu, fd = take(up[:cut], "y", 1), take(down[cut:], "y", -1)
    s2 = swap(jnp.concatenate([line, up, down], axis=0))
    s3 = swap(jnp.concatenate([fu, fd], axis=0))
    own0 = spread_call(at, [line, up, down], ((0, 0, 0, 0, 8), (1, 0, 1, 0, 8), (2, 0, 3, 0, 8)))
    own0 = spread_call(at, [fu, fd], ((0, 0, 2, 0, 4), (1, 0, 2, 4, 4)), own0)
    table = ((0, 0, 0, 0, 8), (0, size, 1, 0, 8), (0, 2 * size, 3, 0, 8), (1, 0, 2, 0, 8))
    other0 = spread_call(at, [s2, s3], table)
    wu, wd, wf = (take(wline, "y", by) for by in (1, -1, 2))
    wo0 = spread_call(
        at, [wline, wu, wd, wf], tuple((i, 0, dy, 0, 8) for i, dy in enumerate((0, 1, 3, 2)))
    )

    def wo0_other():
        (both,) = call(
            functools.partial(cat_kernel, n=4),
            [((WIDTH, CH), BF)],
            [wline, wu, wd, wf],
            scalars=False,
        )
        there = swap(both)
        return spread_call(
            at, [there], tuple((0, n * size, dy, 0, 8) for n, dy in enumerate((0, 1, 3, 2)))
        )

    g = [b1, take(b1, "y", 1), take(b1, "y", 2), take(b1, "y", 3)]
    (near,) = call(near_kernel, [((CH, BUNDLE), BF)], [at, *g])
    p1, m1 = take(near, "z", 1), take(near, "z", -1)
    p2, m2 = take(p1, "z", 1), take(m1, "z", -1)
    p3, m3 = take(p2, "z", 1), take(m2, "z", -1)
    p4 = take(p3, "z", 1)
    chunks = [near, p1, p2, p3, p4, m3, m2, m1]

    par = (small, swap(small))
    blocks = lax.axis_size("z") * lax.axis_size("y")
    pairs = [(2 * i + 1, 2 * (i + 1)) for i in range(blocks - 1)]
    tokens = gather_tokens(state)
    halves, ready = layer_body(0, at, state, tokens, own0, other0, wo0, wo0_other, par, pairs)
    (own1,) = call(
        functools.partial(cat_kernel, n=8),
        [((WIDTH, BUNDLE), BF)],
        [*chunks, ready],
        scalars=False,
    )
    other1 = swap(own1)
    tokens = gather_halves(*halves)
    (state,), _ = layer_body(1, at, halves[0], tokens, own1, other1, own1, other1, par, pairs)
    return state


def solution(mesh):
    torus = Mesh(mesh.devices.reshape(8, 4, 4, 2), SP_TP)
    tp = ("x", "c")
    in_specs = (
        P(SP_TP, None),
        P(),
        P(None, SP, tp),
        P(None, SP, tp),
        P(None, None, tp),
        P(None, tp),
        P(None, tp),
        P(None, tp),
        P(None, tp, SP),
    )
    return jax.shard_map(
        body, mesh=torus, in_specs=in_specs, out_specs=P(SP_TP, None), check_vma=False
    )
```

```python
import functools

import jax
import jax.numpy as jnp
from jax import lax
from jax.experimental import pallas as pl
from jax.experimental.pallas import tpu as pltpu
from jax.sharding import Mesh
from jax.sharding import PartitionSpec as P


SP = ("z", "y")
SP_TP = ("z", "y", "x", "c")
EPS = 1e-06
BF = jnp.bfloat16
F32 = jnp.float32
ROWS = 96
CH = 256
TAPS = 31
KEEP = 32
REST = ROWS - KEEP
WIDTH = 2048
CHANNELS = 2048
BUNDLE = 3 * CH
PIECE = 64


def take(a, axis, by):
    n = lax.axis_size(axis)
    return lax.ppermute(a, axis, [((i + by) % n, i) for i in range(n)])


def swap(a):
    return lax.ppermute(a, "c", [(0, 1), (1, 0)])


def call(kernel, outs, inputs, scratch=(), placed=True, alias=None):
    vmem = pl.BlockSpec(memory_space=pltpu.VMEM)

    def placed_kernel(*refs):
        kernel(tuple(lax.axis_index(a) for a in SP_TP), *refs)

    return pl.pallas_call(
        placed_kernel if placed else kernel,
        out_shape=[jax.ShapeDtypeStruct(s, d) for s, d in outs],
        in_specs=[vmem] * len(inputs),
        out_specs=[vmem] * len(outs),
        scratch_shapes=list(scratch),
        input_output_aliases=alias or {},
        compiler_params=pltpu.CompilerParams(vmem_limit_bytes=12 * 1024 * 1024),
    )(*inputs)


def fold_kernel(at, gain, wv, wg, wo, b0, b1, col):
    sp = at[0] * 4 + at[1]
    for layer, out in ((0, b0), (1, b1)):
        lane = pl.multiple_of((sp // 2) * 128, 128)
        g = gain[layer : layer + 1, pl.ds(lane, 128)]
        col[...] = jnp.broadcast_to(g, (128, 128)).T
        g = col[pl.ds(pl.multiple_of((sp % 2) * PIECE, PIECE), PIECE), 0:1]
        out[:, :CH] = (wv[layer].astype(F32) * g).astype(BF)
        out[:, CH : 2 * CH] = (wg[layer].astype(F32) * g).astype(BF)
        out[:, 2 * CH :] = wo[layer]


def roll_kernel(at, hidden, state):
    for k in range(8):
        src = pl.multiple_of(((at[0] + k) % 8) * CH, CH)
        state[:, k * CH : (k + 1) * CH] = hidden[:, pl.ds(src, CH)]


def par_kernel(cw, cb, cg, cs, par):
    for layer in range(2):
        par[layer, :TAPS] = cw[:, layer]
        for n, a in enumerate((cb, cg, cs)):
            par[layer, TAPS + n : TAPS + n + 1] = a[layer : layer + 1]


def near_kernel(at, a0, a1, a2, a3, out):
    y = at[1]
    for k, a in enumerate((a0, a1, a2, a3)):
        out[pl.ds(pl.multiple_of(((y + k) % 4) * PIECE, PIECE), PIECE)] = a[...]


def line_kernel(own, za, zb, z2, z4, z6, out):
    pieces = (own, za, z2.at[:PIECE], z2.at[PIECE:], z4, z6.at[PIECE:], z6.at[:PIECE], zb)
    for k, a in enumerate(pieces):
        out[k * PIECE : (k + 1) * PIECE] = a[...]


def cat_kernel(*refs):
    out = refs[-1]
    for k, a in enumerate(refs[:8]):
        out[k * CH : (k + 1) * CH] = a[...]


def spread_kernel(at, *refs, table):
    out = refs[-1]
    for i, row, dy, first, n in table:
        base = first * CH + ((at[1] + dy) % 4) * PIECE

        def piece(j, _, i=i, row=row, base=base):
            src = pl.multiple_of(row + j * PIECE, PIECE)
            to = pl.multiple_of(base + j * CH, PIECE)
            out[pl.ds(to, PIECE)] = refs[i][pl.ds(src, PIECE)]
            return 0

        lax.fori_loop(0, n, piece, 0)


def spread_call(arrays, table, into=None):
    inputs = [*arrays] + ([] if into is None else [into])
    return call(
        functools.partial(spread_kernel, table=table),
        [((WIDTH, BUNDLE), BF)],
        inputs,
        alias=None if into is None else {len(inputs) - 1: 0},
    )[0]


def tok_kernel(own, m, f, p, tok, scale):
    for r, a in enumerate((own, m, f, p)):
        tok[r * ROWS : (r + 1) * ROWS] = a[...]
        t = jnp.zeros((ROWS, 128), F32)
        for k in range(WIDTH // 128):
            v = a[:, k * 128 : (k + 1) * 128].astype(F32)
            t = t + v * v
        s = lax.rsqrt(jnp.sum(t, axis=1, keepdims=True) * (1.0 / WIDTH) + EPS)
        scale[r * ROWS : (r + 1) * ROWS] = jnp.broadcast_to(s, (ROWS, 128))


def glu_of(tok, scale, w):
    both = jnp.dot(tok[...], w[:, : 2 * CH], preferred_element_type=F32)
    s = scale[:, 0:1]
    lin, gate = both[:, :CH] * s, both[:, CH:] * s
    return (lin / (1.0 + jnp.exp(-gate))).astype(BF)


def glu_first_kernel(tok, scale, w, glu):
    glu[...] = glu_of(tok, scale, w)


def glu_second_kernel(at, tok, scale, other, w, glu, tails, last):
    glu[...] = glu_of(tok, scale, w)
    for r in range(4):
        here = slice((r + 1) * ROWS - KEEP, (r + 1) * ROWS)
        tails[r * KEEP : (r + 1) * KEEP, :CH] = other[here]
        tails[r * KEEP : (r + 1) * KEEP, CH:] = glu[here]
    last[...] = tails[pl.ds(pl.multiple_of(((at[2] + 1) % 4) * KEEP, KEEP), KEEP)]


def glu_calls(tokens, own, other):
    size = (4 * ROWS, CH)
    tok, scale = call(
        tok_kernel, [((4 * ROWS, WIDTH), BF), ((4 * ROWS, 128), F32)], list(tokens), placed=False
    )
    (glu_a,) = call(glu_first_kernel, [(size, BF)], [tok, scale, own], placed=False)
    glu_b, tails, last = call(
        glu_second_kernel,
        [(size, BF), ((4 * KEEP, 2 * CH), BF), ((KEEP, 2 * CH), BF)],
        [tok, scale, glu_a, other],
    )
    return glu_a, glu_b, tails, last


def conv_strip(win, par, lanes, rows):
    acc = jnp.zeros((rows, 128), F32) + par[TAPS : TAPS + 1, lanes]
    for s in range(8):
        shifted = win[s : s + rows + (24 if s else 32)]
        for base in range(0, 40, 8):
            tap = base + s - (KEEP - (TAPS - 1))
            if 0 <= tap < TAPS:
                acc = acc + par[tap : tap + 1, lanes] * shifted[base : base + rows]
    return acc


def conv_rest_kernel(glu_a, glu_b, par_a, par_b, mixed, t1, t2, win, *, layer):
    par_a, par_b = par_a.at[layer], par_b.at[layer]

    def block(r, _):
        here = pl.multiple_of(r * ROWS, KEEP)
        s1 = jnp.zeros((REST, 128), F32)
        s2 = jnp.zeros((REST, 128), F32)
        for strip in range(4):
            lanes = slice((strip % 2) * 128, (strip % 2) * 128 + 128)
            glu, par = (glu_a, par_a) if strip < 2 else (glu_b, par_b)
            win[...] = glu[pl.ds(here, ROWS), lanes].astype(F32)
            acc = conv_strip(win, par, lanes, REST)
            mixed[pl.ds(pl.multiple_of(r * REST, REST), REST), strip * 128 : strip * 128 + 128] = acc
            s1 = s1 + acc
            s2 = s2 + acc * acc
        t1[pl.ds(pl.multiple_of(r * REST, REST), REST)] = s1
        t2[pl.ds(pl.multiple_of(r * REST, REST), REST)] = s2
        return 0

    lax.fori_loop(0, 4, block, 0)


def conv_edge_kernel(at, glu_a, glu_b, other, before, par_a, par_b, t1, t2, mixed, stats, win, l1, l2, *, layer):
    par_a, par_b = par_a.at[layer], par_b.at[layer]
    x, c = at[2], at[3]

    def block(r, _):
        idx = jnp.where(c == 1, r, (r + 1) % 4)
        first = jnp.logical_and(c == 0, r == x)
        here = pl.multiple_of(r * ROWS, KEEP)
        edge_at = pl.multiple_of(idx * KEEP, KEEP)
        s1 = jnp.zeros((KEEP, 128), F32)
        s2 = jnp.zeros((KEEP, 128), F32)
        for strip in range(4):
            lanes = slice((strip % 2) * 128, (strip % 2) * 128 + 128)
            there = slice(((strip + 2) % 4) * 128, ((strip + 2) % 4) * 128 + 128)
            glu, par = (glu_a, par_a) if strip < 2 else (glu_b, par_b)
            edge = other[pl.ds(edge_at, KEEP), there].astype(F32)
            win[0:KEEP] = jnp.where(first, before[:, there].astype(F32), edge)
            win[KEEP:] = glu[pl.ds(here, KEEP), lanes].astype(F32)
            acc = conv_strip(win, par, lanes, KEEP)
            mixed[pl.ds(pl.multiple_of(r * KEEP, KEEP), KEEP), strip * 128 : strip * 128 + 128] = acc
            s1 = s1 + acc
            s2 = s2 + acc * acc
        l1[pl.ds(pl.multiple_of(r * KEEP, KEEP), KEEP)] = s1
        l2[pl.ds(pl.multiple_of(r * KEEP, KEEP), KEEP)] = s2
        return 0

    lax.fori_loop(0, 4, block, 0)
    for o, low, high in ((0, l1, t1), (4, l2, t2)):
        for r in range(4):
            rows = [low[r * KEEP : (r + 1) * KEEP], high[r * REST : (r + 1) * REST]]
            rows = jnp.concatenate(rows + [jnp.zeros((128 - ROWS, 128), F32)], axis=0)
            stats[o + r : o + r + 1] = jnp.sum(rows.T, axis=0, keepdims=True)


def out_kernel(*refs, blocks, layer):
    at, low, high, stats, par_a, par_b, wa, wb = refs[:8]
    outs, act = refs[8:-1], refs[-1]
    par_a, par_b = par_a.at[layer], par_b.at[layer]
    x = at[2]
    own, m, f, p = (stats[pl.ds(pl.multiple_of(((x + d) % 4) * 8, 8), 8)] for d in (0, 3, 2, 1))
    rows = []
    for o in (0, 4):
        for r in range(4):
            i, j, k = o + (r - 1) % 4, o + (r + 2) % 4, o + (r + 1) % 4
            rows.append(own[o + r : o + r + 1] + m[i : i + 1] + f[j : j + 1] + p[k : k + 1])
    mean = jnp.concatenate(rows[:4], axis=0) * (1.0 / CHANNELS)
    msq = jnp.concatenate(rows[4:], axis=0) * (1.0 / CHANNELS)
    inv = lax.rsqrt(msq - mean * mean + EPS)
    cols = jnp.concatenate([mean, inv], axis=0).T
    for n, r in enumerate(blocks):
        for src, size, first in ((low, KEEP, 0), (high, REST, KEEP)):
            mu = cols[first : first + size, r : r + 1]
            iv = cols[first : first + size, 4 + r : 5 + r]
            for s, par in ((0, par_a), (1, par_b)):
                v = (src[r * size : (r + 1) * size, s * CH : (s + 1) * CH] - mu) * iv
                v = v * par[TAPS + 1 : TAPS + 2] + par[TAPS + 2 : TAPS + 3]
                to = n * ROWS + first
                act[to : to + size, s * CH : (s + 1) * CH] = (v / (1.0 + jnp.exp(-v))).astype(BF)
    dims = (((1,), (1,)), ((), ()))
    d = lax.dot_general(act[:, :CH], wa[:, 2 * CH :], dims, preferred_element_type=F32)
    d = d + lax.dot_general(act[:, CH:], wb[:, 2 * CH :], dims, preferred_element_type=F32)
    for n, out in enumerate(outs):
        out[...] = d[n * ROWS : (n + 1) * ROWS].astype(out.dtype)


def add_kernel(at, h, o0, m, p, f, out, *, last):
    for k in range(8):
        src = slice(k * CH, (k + 1) * CH)
        t = o0[:, src] + m[:, src].astype(F32) + p[:, src].astype(F32) + f[:, src].astype(F32)
        t = (h[:, src].astype(F32) + t).astype(BF)
        if last:
            out[:, pl.ds(pl.multiple_of(((at[0] + k) % 8) * CH, CH), CH)] = t
        else:
            out[:, src] = t


def out_call(layer, blocks, kinds, *inputs):
    return call(
        functools.partial(out_kernel, blocks=blocks, layer=layer),
        [((ROWS, WIDTH), k) for k in kinds],
        list(inputs),
        [pltpu.VMEM((len(blocks) * ROWS, 2 * CH), BF)],
    )


def layer_body(layer, state, tokens, own, other, par, before_pairs):
    glu_a, glu_b, tails, last = glu_calls(tokens, own, other)
    there = swap(tails)
    before = lax.ppermute(last, ("z", "y", "c"), before_pairs)
    par_a, par_b = par
    high, t1, t2 = call(
        functools.partial(conv_rest_kernel, layer=layer),
        [((4 * REST, 2 * CH), F32)] + [((4 * REST, 128), F32)] * 2,
        [glu_a, glu_b, par_a, par_b],
        [pltpu.VMEM((ROWS, 128), F32)],
        placed=False,
    )
    low, s = call(
        functools.partial(conv_edge_kernel, layer=layer),
        [((4 * KEEP, 2 * CH), F32), ((8, 128), F32)],
        [glu_a, glu_b, there, before, par_a, par_b, t1, t2],
        [pltpu.VMEM((2 * KEEP, 128), F32)] + [pltpu.VMEM((4 * KEEP, 128), F32)] * 2,
    )
    stats = lax.all_to_all(jnp.broadcast_to(s[None], (4, 8, 128)), "x", 0, 0, tiled=True)
    inputs = (low, high, stats.reshape(32, 128), par_a, par_b, own, other)
    (o2,) = out_call(layer, (2,), (BF,), *inputs)
    from_f = take(o2, "x", 2)
    o3, o1, o0 = out_call(layer, (3, 1, 0), (BF, BF, F32), *inputs)
    from_m, from_p = take(o3, "x", -1), take(o1, "x", 1)
    (state,) = call(
        functools.partial(add_kernel, last=layer == 1),
        [((ROWS, WIDTH), BF)],
        [state, o0, from_m, from_p, from_f],
    )
    return state, o1


def gather_tokens(h):
    m, p, f = take(h, "x", -1), take(h, "x", 1), take(h, "x", 2)
    return h, m, f, p


def body(hidden, norm_gain, w_value, w_gate, conv_weight, conv_bias, chan_gain, chan_shift, w_out):
    b0, b1 = call(
        fold_kernel,
        [((PIECE, BUNDLE), BF)] * 2,
        [norm_gain, w_value, w_gate, w_out.swapaxes(1, 2)],
        [pltpu.VMEM((128, 128), F32)],
    )
    (state,) = call(roll_kernel, [((ROWS, WIDTH), BF)], [hidden])
    (small,) = call(
        par_kernel,
        [((2, 40, CH), F32)],
        [conv_weight.swapaxes(0, 1), conv_bias, chan_gain, chan_shift],
        placed=False,
    )

    za, zb, z4 = take(b0, "z", 1), take(b0, "z", -1), take(b0, "z", 4)
    z2 = take(jnp.concatenate([b0, za], axis=0), "z", 2)
    z6 = take(jnp.concatenate([b0, zb], axis=0), "z", -2)
    size, cut = 8 * PIECE, 4 * PIECE
    (line,) = call(line_kernel, [((size, BUNDLE), BF)], [b0, za, zb, z2, z4, z6], placed=False)
    up, down = take(line, "y", 1), take(line, "y", -1)
    fu, fd = take(up[:cut], "y", 1), take(down[cut:], "y", -1)
    s2 = swap(jnp.concatenate([line, up, down], axis=0))
    s3 = swap(jnp.concatenate([fu, fd], axis=0))
    own0 = spread_call([line, up, down], ((0, 0, 0, 0, 8), (1, 0, 1, 0, 8), (2, 0, 3, 0, 8)))
    own0 = spread_call([fu, fd], ((0, 0, 2, 0, 4), (1, 0, 2, 4, 4)), own0)
    table = ((0, 0, 0, 0, 8), (0, size, 1, 0, 8), (0, 2 * size, 3, 0, 8), (1, 0, 2, 0, 8))
    other0 = spread_call([s2, s3], table)

    g = [b1, take(b1, "y", 1), take(b1, "y", 2), take(b1, "y", 3)]
    (near,) = call(near_kernel, [((CH, BUNDLE), BF)], [*g])
    p1, m1 = take(near, "z", 1), take(near, "z", -1)
    p2, m2 = take(p1, "z", 1), take(m1, "z", -1)
    p3, m3 = take(p2, "z", 1), take(m2, "z", -1)
    p4 = take(p3, "z", 1)
    chunks = [near, p1, p2, p3, p4, m3, m2, m1]

    par = (small, swap(small))
    size = lax.axis_size("z") * lax.axis_size("y")
    pairs = [(2 * i + 1, 2 * (i + 1)) for i in range(size - 1)]
    state, ready = layer_body(0, state, gather_tokens(state), own0, other0, par, pairs)
    (own1,) = call(cat_kernel, [((WIDTH, BUNDLE), BF)], [*chunks, ready], placed=False)
    other1 = swap(own1)
    state, _ = layer_body(1, state, gather_tokens(state), own1, other1, par, pairs)
    return state


def solution(mesh):
    torus = Mesh(mesh.devices.reshape(8, 4, 4, 2), SP_TP)
    tp = ("x", "c")
    in_specs = (
        P(SP_TP, None),
        P(),
        P(None, SP, tp),
        P(None, SP, tp),
        P(None, None, tp),
        P(None, tp),
        P(None, tp),
        P(None, tp),
        P(None, tp, SP),
    )
    return jax.shard_map(
        body, mesh=torus, in_specs=in_specs, out_specs=P(SP_TP, None), check_vma=False
    )
```
